256 devices in a mesh: sp: 32 (over z, x), tp: 8 (over y, core).
Axes of the slice: x: 4, y: 4, z: 8, core: 2. Of those that a mesh axis runs over, the one named last changes fastest.
Arguments:
- latents: bfloat16 [16384, 2048], P(('sp', 'tp')), may hold values from -6 to 6
- context: bfloat16 [512, 2048], P('sp'), may hold values from -6 to 6
- cond: float32 [2048], P('sp'), may hold values from -6 to 6
- ctx_cond: float32 [2048], P('sp'), may hold values from -6 to 6
- mod_weight: float32 [2048, 6144], P('sp', 'tp'), may hold values from -0.125 to 0.125
- query_weight: bfloat16 [2048, 2048], P(None, 'tp'), may hold values from -1 to 1, as said below
- key_matrix: bfloat16 [2048, 1024], P(None, 'tp'), may hold values from -1 to 1, as said below
- value_matrix: bfloat16 [2048, 1024], P(None, 'tp'), may hold values from -0.125 to 0.125
- out_weight: bfloat16 [2048, 2048], P('tp'), may hold values from -0.125 to 0.125
- query_gain: float32 [128], replicated, may hold values from 0.7 to 7
- key_gain: float32 [128], replicated, may hold values from 0.7 to 7
Outputs:
- updated: bfloat16 [16384, 2048], P(('sp', 'tp'))
The draws below stay inside these ranges and needn't reach their ends.
Inputs may be any that keep to these rules, and one draw needn't show every extreme that they name: `query_weight`: entries of order 2048 to the power -1/2. `key_matrix`: entries of order 2048 to the power -1/2.
All inputs are finite; a program needn't handle non-finite values.
Results may differ from the reference program's by a relative error of at most 0.0085.
The reference program's roundings to bfloat16 on the way count: a program that leaves them out, or rounds other values in their place, can miss the bound.
Values may be sent and summed in bfloat16 or wider, within the bound.
A program may use at most 128 MiB of HBM per device.

```python
import math
import jax
import jax.numpy as jnp
from jax import lax

MODEL_DIM = 2048
HEAD_SIZE = 128
QUERY_HEAD_COUNT = 16
KEY_VALUE_HEADS = 8
GRID_W = 64
CTX = 512
TOKENS = 16384


def paired_weights(key):
    query_base = jax.random.normal(jax.random.fold_in(key, 11), (MODEL_DIM, QUERY_HEAD_COUNT * HEAD_SIZE), jnp.float32) * MODEL_DIM ** (-0.5)
    key_start = jax.random.normal(jax.random.fold_in(key, 12), (MODEL_DIM, KEY_VALUE_HEADS * HEAD_SIZE), jnp.float32) * MODEL_DIM ** (-0.5)
    return (query_base, key_start)


def draw_query_weight(key, part):
    return paired_weights(key)[0].astype(jnp.bfloat16)


def draw_key_matrix(key, part):
    return paired_weights(key)[1].astype(jnp.bfloat16)


def draw_query_gain(key, part):
    return jax.random.uniform(jax.random.fold_in(key, 21), (HEAD_SIZE,), jnp.float32, 0.7, 1.3)


def draw_key_gain(key, part):
    return jax.random.uniform(jax.random.fold_in(key, 22), (HEAD_SIZE,), jnp.float32, 0.7, 1.3)


def shard_levels(rng, dims, shards, smallest, high):
    loudness, own = 1.0, jax.random.fold_in(rng, 6)
    for position, parts in shards:
        draws = jnp.exp(jax.random.uniform(jax.random.fold_in(own, position), (parts,), jnp.float32, smallest / len(shards), high / len(shards)))
        loudness = loudness * jnp.repeat(draws, dims[position] // parts).reshape([-1 if axis == position else 1 for axis in range(len(dims))])
    return loudness


def centred(stream_key, dims, width, most, pieces=(), kind=jnp.bfloat16):
    result = jax.random.normal(stream_key, dims, jnp.float32) * width
    if len(pieces) > 0:
        result = shard_levels(stream_key, dims, pieces, -0.22, 0.18) * result
    return jnp.clip(result, min=-most, max=most).astype(kind)


def setup_inputs(seed: int = 0) -> dict:
    key_of = jax.random.split(jax.random.key(seed), 12)
    latents = centred(key_of[0], (TOKENS, MODEL_DIM), 1.0, 6.0, ((0, 256),))
    context = centred(key_of[1], (CTX, MODEL_DIM), 1.0, 6.0, ((0, 32),))
    cond = centred(key_of[2], (MODEL_DIM,), 1.0, 6.0, ((0, 32),), jnp.float32)
    ctx_cond = centred(key_of[3], (MODEL_DIM,), 1.0, 6.0, ((0, 32),), jnp.float32)
    mod_weight = centred(key_of[4], (MODEL_DIM, 3 * MODEL_DIM), MODEL_DIM ** -0.5, 0.125, ((0, 32), (1, 8)), jnp.float32)
    query_weight = draw_query_weight(jax.random.fold_in(key_of[11], 71), 0)
    key_matrix = draw_key_matrix(jax.random.fold_in(key_of[11], 71), 0)
    value_matrix = centred(key_of[7], (MODEL_DIM, KEY_VALUE_HEADS * HEAD_SIZE), MODEL_DIM ** -0.5, 0.125, ((1, 8),))
    out_weight = centred(key_of[8], (QUERY_HEAD_COUNT * HEAD_SIZE, MODEL_DIM), (QUERY_HEAD_COUNT * HEAD_SIZE) ** -0.5, 0.125, ((0, 8),))
    query_gain = draw_query_gain(jax.random.fold_in(key_of[11], 71), 0)
    key_gain = draw_key_gain(jax.random.fold_in(key_of[11], 71), 0)
    return {"latents": latents, "context": context, "cond": cond, "ctx_cond": ctx_cond, "mod_weight": mod_weight, "query_weight": query_weight, "key_matrix": key_matrix, "value_matrix": value_matrix, "out_weight": out_weight, "query_gain": query_gain, "key_gain": key_gain}


NORM_EPS = 1e-06
ROPE_BASE = 10000.0

def normalize(latent_value_rows):
    return latent_value_rows * lax.rsqrt(lax.optimization_barrier(jnp.mean(latent_value_rows * latent_value_rows, axis=-1, keepdims=True)) + NORM_EPS)

def rotate(latent_value_rows, positions):
    quarter = latent_value_rows.shape[-1] // 2
    inv_freq = ROPE_BASE ** (-jnp.arange(quarter, dtype=jnp.float32) / quarter)
    angles = positions.astype(jnp.float32)[:, None] * inv_freq[None, :]
    cos_table = jnp.cos(angles)[:, None, :]
    sin_table = jnp.sin(angles)[:, None, :]
    first, second = (latent_value_rows[..., :quarter], latent_value_rows[..., quarter:])
    return jnp.concatenate([first * cos_table - second * sin_table, second * cos_table + first * sin_table], axis=-1)

def axial(latent_value_rows, positions):
    half_dim = latent_value_rows.shape[-1] // 2
    return jnp.concatenate([rotate(latent_value_rows[..., :half_dim], positions // GRID_W), rotate(latent_value_rows[..., half_dim:], positions % GRID_W)], axis=-1)

def modulate(latent_value_rows, mod_row):
    model_width = latent_value_rows.shape[-1]
    shift_vec = mod_row[:model_width]
    scale_vec = mod_row[model_width:2 * model_width]
    return (normalize(latent_value_rows.astype(jnp.float32)) * (1.0 + scale_vec) + shift_vec).astype(jnp.bfloat16)

def reference(latents, context, cond, ctx_cond, mod_weight, query_weight, key_matrix, value_matrix, out_weight, query_gain, key_gain):
    model_width = latents.shape[1]
    latent_count = latents.shape[0]
    prefix_count = context.shape[0]
    modulation = jnp.dot(jax.nn.silu(jnp.stack([cond, ctx_cond])), mod_weight, precision=lax.Precision.HIGHEST)
    gate_vec = modulation[0, 2 * model_width:]
    normalised_rows = modulate(latents, modulation[0])
    prefix_normalised = modulate(context, modulation[1])
    positions = jnp.arange(latent_count, dtype=jnp.int32)
    query_rows = jnp.dot(normalised_rows, query_weight, preferred_element_type=jnp.float32).reshape(latent_count, QUERY_HEAD_COUNT, HEAD_SIZE)
    query_rows = axial(normalize(query_rows) * query_gain, positions).astype(jnp.bfloat16)
    latent_key_rows = jnp.dot(normalised_rows, key_matrix, preferred_element_type=jnp.float32).reshape(latent_count, KEY_VALUE_HEADS, HEAD_SIZE)
    latent_key_rows = axial(normalize(latent_key_rows) * key_gain, positions).astype(jnp.bfloat16)
    latent_value_rows = jnp.dot(normalised_rows, value_matrix, preferred_element_type=jnp.float32).reshape(latent_count, KEY_VALUE_HEADS, HEAD_SIZE).astype(jnp.bfloat16)
    prefix_keys = jnp.dot(prefix_normalised, key_matrix, preferred_element_type=jnp.float32).reshape(prefix_count, KEY_VALUE_HEADS, HEAD_SIZE)
    prefix_keys = (normalize(prefix_keys) * key_gain).astype(jnp.bfloat16)
    prefix_values = jnp.dot(prefix_normalised, value_matrix, preferred_element_type=jnp.float32).reshape(prefix_count, KEY_VALUE_HEADS, HEAD_SIZE).astype(jnp.bfloat16)
    keys_all = jnp.concatenate([prefix_keys, latent_key_rows], axis=0).astype(jnp.float32)
    values_all = jnp.concatenate([prefix_values, latent_value_rows], axis=0).astype(jnp.float32)
    lift = math.log(latent_count / (2.0 * prefix_count))
    lift_row = jnp.concatenate([jnp.full((prefix_count,), lift, jnp.float32), jnp.zeros((latent_count,), jnp.float32)])
    group_size = QUERY_HEAD_COUNT // KEY_VALUE_HEADS
    rows_per_block = math.gcd(latent_count, 256)
    token_blocks = query_rows.reshape(latent_count // rows_per_block, rows_per_block, KEY_VALUE_HEADS, group_size, HEAD_SIZE)
    inv_root = HEAD_SIZE ** (-0.5)

    def one_block(block):
        scores = jnp.einsum('qhgd,khd->hgqk', block.astype(jnp.float32), keys_all) * inv_root + lift_row
        top_row = lax.optimization_barrier(jnp.max(scores, axis=-1, keepdims=True))
        weights = jnp.exp(scores - top_row)
        total = lax.optimization_barrier(jnp.sum(weights, axis=-1))
        probs = lax.optimization_barrier(weights.astype(jnp.bfloat16)).astype(jnp.float32)
        summed = jnp.einsum('hgqk,khd->qhgd', probs, values_all)
        return (summed / jnp.transpose(total, (2, 0, 1))[..., None]).astype(jnp.bfloat16)
    attended = lax.map(one_block, token_blocks).reshape(latent_count, QUERY_HEAD_COUNT * HEAD_SIZE)
    mixed = jnp.dot(attended, out_weight, preferred_element_type=jnp.float32)
    return (latents.astype(jnp.float32) + gate_vec * normalize(mixed)).astype(jnp.bfloat16)
```

```python
import functools
import math

import jax
import jax.numpy as jnp
import numpy as np
from jax import lax
from jax.experimental import pallas as pl
from jax.experimental.pallas import tpu as pltpu
from jax.sharding import Mesh
from jax.sharding import PartitionSpec as P

GRID_W = 64
NORM_EPS = 1e-06
ROPE_BASE = 10000.0
Z, X, Y, C = 8, 4, 4, 2
AXES = ("z", "x", "y", "c")
SP = ("z", "x")
TP = ("y", "c")
MESH = pl.DeviceIdType.MESH
D = 2048
HEAD = 128
ROWS = 64
CTX_ROWS = 16
GROUP_ROWS = ROWS * Y * C
UNIT = CTX_ROWS + GROUP_ROWS
TOTAL_KEYS = UNIT * Z * X
LIFT = 16.0
SCORE_SCALE = HEAD ** (-0.5) * math.log2(math.e)


def coords():
    return tuple(lax.axis_index(a) for a in AXES)


def remote(src, dst, send, recv, dev):
    return pltpu.make_async_remote_copy(
        src_ref=src, dst_ref=dst, send_sem=send, recv_sem=recv, device_id=dev, device_id_type=MESH
    )


def meet(peers):
    barrier = pltpu.get_barrier_semaphore()
    for dev in peers:
        pl.semaphore_signal(barrier, inc=1, device_id=dev, device_id_type=MESH)
    pl.semaphore_wait(barrier, len(peers))


def rope_tables():
    quarter = HEAD // 4
    freq = (np.float32(ROPE_BASE) ** (-np.arange(quarter, dtype=np.float32) / np.float32(quarter))).astype(np.float32)
    lanes = freq[np.arange(HEAD) % quarter]
    sign = np.where(np.arange(HEAD) % (HEAD // 2) < quarter, -1.0, 1.0)
    grid_rows = GROUP_ROWS * Z * X // GRID_W
    row_angle = (np.arange(grid_rows, dtype=np.float32)[:, None] * lanes[None]).astype(np.float64)
    col_angle = (np.arange(GRID_W, dtype=np.float32)[:, None] * lanes[None]).astype(np.float64)
    as32 = lambda a: jnp.asarray(a.astype(np.float32))
    return (
        as32(np.cos(row_angle)),
        as32(np.sin(row_angle) * sign),
        as32(np.cos(col_angle)),
        as32(np.sin(col_angle) * sign),
    )


def column(row):
    n = row.shape[1]
    eye = lax.broadcasted_iota(jnp.int32, (n, n), 0) == lax.broadcasted_iota(jnp.int32, (n, n), 1)
    return jnp.sum(jnp.where(eye, row, 0.0), axis=1, keepdims=True)


def front_kernel(
    lat, ctx, cond, ctx_cond, modw, wq, wk, wv, q_gain, k_gain, cos_r, sin_r, cos_c, sin_c,
    q_out, kv_out, gate_out,
    xg, ws, cr, sr, part, x_in, x_sum, z_in, mod, xn, proj,
    w_sem, lat_send, lat_recv, x_send, x_recv, z_send, z_recv, t_send, t_recv,
):
    z, x, y, c = coords()
    me = y * C + c
    sp = z * X + x
    up, down = lax.rem(y + 1, Y), lax.rem(y + Y - 1, Y)
    far = lax.rem(y + 2, Y)
    loads = [
        pltpu.make_async_copy(wq, ws.at[:, pl.ds(0, 2 * HEAD)], w_sem.at[0]),
        pltpu.make_async_copy(wk, ws.at[:, pl.ds(2 * HEAD, HEAD)], w_sem.at[1]),
        pltpu.make_async_copy(wv, ws.at[:, pl.ds(3 * HEAD, HEAD)], w_sem.at[2]),
        pltpu.make_async_copy(cos_r.at[pl.ds(sp * 8, 8)], cr, w_sem.at[3]),
        pltpu.make_async_copy(sin_r.at[pl.ds(sp * 8, 8)], sr, w_sem.at[4]),
    ]
    for copy in loads:
        copy.start()
    x_peers = [(z, lax.rem(x + r, X), y, c) for r in range(1, X)]
    z_peers = [(lax.rem(z + r, Z), x, y, c) for r in range(1, Z)]
    t_rel = [(ry, rc) for ry in range(Y) for rc in range(C) if (ry, rc) != (0, 0)]
    t_peers = [(z, x, lax.rem(y + ry, Y), c + rc * (1 - 2 * c)) for ry, rc in t_rel]
    sib = (z, x, y, 1 - c)
    meet(x_peers + z_peers + t_peers)

    def slot(yy, cc):
        return yy * C + cc

    sends = []

    def send_lat(i, src, yy, cc, dev, lo=0, n=ROWS):
        copy = remote(src, xg.at[slot(yy, cc), pl.ds(lo, n)], lat_send.at[i], lat_recv.at[i], dev)
        copy.start()
        sends.append(copy)
        return copy

    up_dev, down_dev = (z, x, up, c), (z, x, down, c)
    c0 = send_lat(0, lat, y, c, up_dev)
    c1 = send_lat(1, lat, y, c, down_dev)
    c2 = send_lat(2, lat, y, c, sib)

    w = modw[...]
    for r, vec in enumerate((cond, ctx_cond)):
        v = vec[...]
        v = column(v * lax.logistic(v))
        row = jnp.sum(v * w, axis=0, keepdims=True)
        for i in range(6):
            part[r * 6 + i : r * 6 + i + 1, :] = row[:, i * HEAD : (i + 1) * HEAD]
    part[12:16, :] = jnp.zeros((4, HEAD), jnp.float32)
    xg[me] = lat[...]

    xs = [remote(part, x_in.at[i], x_send.at[i], x_recv.at[i], d) for i, d in enumerate(x_peers)]
    for s in xs:
        s.start()
    for s in xs:
        s.wait_recv()
    x_sum[...] = part[...] + x_in[0] + x_in[1] + x_in[2]
    zs = [remote(x_sum, z_in.at[i], z_send.at[i], z_recv.at[i], d) for i, d in enumerate(z_peers)]
    for s in zs:
        s.start()

    half = ROWS // 2
    c0.wait_recv()
    c3 = send_lat(3, xg.at[slot(down, c), pl.ds(0, half)], down, c, up_dev, 0, half)
    c5 = send_lat(5, xg.at[slot(down, c)], down, c, sib)
    c1.wait_recv()
    c4 = send_lat(4, xg.at[slot(up, c), pl.ds(half, half)], up, c, down_dev, half, half)
    c6 = send_lat(6, xg.at[slot(up, c)], up, c, sib)

    for s in zs:
        s.wait_recv()
    total = x_sum[...]
    for i in range(Z - 1):
        total = total + z_in[i]
    mod[me] = total
    ts = [remote(mod.at[me], mod.at[me], t_send.at[i], t_recv.at[i], d) for i, d in enumerate(t_peers)]
    for s in ts:
        s.start()
    c3.wait_recv()
    c4.wait_recv()
    c7 = send_lat(7, xg.at[slot(far, c)], far, c, sib)
    for copy in loads:
        copy.wait()
    for s in ts:
        s.wait_recv()

    def mod_row(r, first):
        tiles = [first + t for t in range(D // HEAD)]
        return jnp.concatenate([mod[t // 6, r * 6 + t % 6 : r * 6 + t % 6 + 1, :] for t in tiles], axis=1)

    gate_out[...] = mod_row(0, 32)

    def modulated(rows, r):
        v = rows.astype(jnp.float32)
        v = v * lax.rsqrt(jnp.mean(v * v, axis=-1, keepdims=True) + NORM_EPS)
        return (v * (1.0 + mod_row(r, 16)) + mod_row(r, 0)).astype(jnp.bfloat16)

    xn[:CTX_ROWS, :] = modulated(ctx[...], 1)
    for s in (c2, c5, c6, c7):
        s.wait_recv()
    for j in range(Y * C):
        xn[CTX_ROWS + ROWS * j : CTX_ROWS + ROWS * (j + 1), :] = modulated(xg[j], 0)

    lane = lax.broadcasted_iota(jnp.int32, (GRID_W, HEAD), 1)
    is_row = lane < HEAD // 2
    is_first = lax.rem(lane, HEAD // 2) < HEAD // 4

    def unit_rows(v, gain):
        return v * lax.rsqrt(jnp.mean(v * v, axis=-1, keepdims=True) + NORM_EPS) * gain

    for lo, n in ((0, UNIT // 2 + 8), (UNIT // 2 + 8, UNIT // 2 - 8)):
        proj[lo : lo + n, :] = jnp.dot(xn[lo : lo + n, :], ws[...], preferred_element_type=jnp.float32)
    qg, kg = q_gain[...], k_gain[...]
    kv_out[:CTX_ROWS, :HEAD] = unit_rows(proj[:CTX_ROWS, 2 * HEAD : 3 * HEAD], kg).astype(jnp.bfloat16)
    kv_out[:CTX_ROWS, HEAD:] = proj[:CTX_ROWS, 3 * HEAD :].astype(jnp.bfloat16) * jnp.bfloat16(LIFT)
    for j in range(GROUP_ROWS // GRID_W):
        lo = CTX_ROWS + GRID_W * j
        cos = jnp.where(is_row, cr[j : j + 1, :], cos_c[...])
        sin = jnp.where(is_row, sr[j : j + 1, :], sin_c[...])

        def turned(v, gain):
            v = unit_rows(v, gain)
            other = jnp.where(is_first, pltpu.roll(v, HEAD - HEAD // 4, 1), pltpu.roll(v, HEAD // 4, 1))
            return (v * cos + other * sin).astype(jnp.bfloat16)

        for h in range(2):
            q_out[GRID_W * j : GRID_W * (j + 1), h * HEAD : (h + 1) * HEAD] = turned(
                proj[lo : lo + GRID_W, h * HEAD : (h + 1) * HEAD], qg
            )
        kv_out[lo : lo + GRID_W, :HEAD] = turned(proj[lo : lo + GRID_W, 2 * HEAD : 3 * HEAD], kg)
        kv_out[lo : lo + GRID_W, HEAD:] = proj[lo : lo + GRID_W, 3 * HEAD :].astype(jnp.bfloat16)

    for s in sends + xs + zs + ts:
        s.wait_send()


def front(latents, context, cond, ctx_cond, mod_weight, wq, wk, wv, q_gain, k_gain):
    vm = pl.BlockSpec(memory_space=pltpu.VMEM)
    hbm = pl.BlockSpec(memory_space=pl.ANY)
    cos_r, sin_r, cos_c, sin_c = rope_tables()
    bf, f32 = jnp.bfloat16, jnp.float32
    dma = pltpu.SemaphoreType.DMA
    return pl.pallas_call(
        front_kernel,
        name="front",
        out_shape=(
            jax.ShapeDtypeStruct((GROUP_ROWS, 2 * HEAD), bf),
            jax.ShapeDtypeStruct((UNIT, 2 * HEAD), bf),
            jax.ShapeDtypeStruct((1, D), f32),
        ),
        in_specs=[vm] * 5 + [hbm] * 3 + [vm] * 2 + [hbm] * 2 + [vm] * 2,
        out_specs=(vm, vm, vm),
        scratch_shapes=[
            pltpu.VMEM((Y * C, ROWS, D), bf),
            pltpu.VMEM((D, 4 * HEAD), bf),
            pltpu.VMEM((8, HEAD), f32),
            pltpu.VMEM((8, HEAD), f32),
            pltpu.VMEM((16, HEAD), f32),
            pltpu.VMEM((X - 1, 16, HEAD), f32),
            pltpu.VMEM((16, HEAD), f32),
            pltpu.VMEM((Z - 1, 16, HEAD), f32),
            pltpu.VMEM((Y * C, 16, HEAD), f32),
            pltpu.VMEM((UNIT, D), bf),
            pltpu.VMEM((UNIT, 4 * HEAD), f32),
            dma((5,)), dma((8,)), dma((8,)), dma((X - 1,)), dma((X - 1,)),
            dma((Z - 1,)), dma((Z - 1,)), dma((7,)), dma((7,)),
        ],
        compiler_params=pltpu.CompilerParams(collective_id=0, has_side_effects=True, vmem_limit_bytes=40 << 20),
    )(
        latents, context, cond.reshape(1, -1), ctx_cond.reshape(1, -1), mod_weight, wq, wk, wv,
        q_gain.reshape(1, -1), k_gain.reshape(1, -1), cos_r, sin_r, cos_c, sin_c,
    )


def flash_kernel(steps, sub, q_ref, kv_ref, o_ref, m_ref, acc_ref):
    i = pl.program_id(0)
    keys = kv_ref.shape[0]
    rows = q_ref.shape[0]

    @pl.when(i == 0)
    def _():
        m_ref[...] = jnp.full_like(m_ref, -1e30)
        acc_ref[...] = jnp.zeros_like(acc_ref)

    k = kv_ref[:, :HEAD]
    row = lax.broadcasted_iota(jnp.int32, (keys, HEAD), 0) + i * keys
    ones = jnp.where(lax.rem(row, UNIT) < CTX_ROWS, LIFT, 1.0).astype(jnp.bfloat16)
    v = jnp.concatenate([kv_ref[:, HEAD:], ones], axis=1)
    for h in range(2):
        for r in range(0, rows, sub):
            at = pl.ds(h * rows + r, sub)
            s = lax.dot_general(
                q_ref[r : r + sub, h * HEAD : (h + 1) * HEAD], k, (((1,), (1,)), ((), ())),
                preferred_element_type=jnp.float32,
            )
            m_old = m_ref[at, :]
            m_new = jnp.maximum(m_old, jnp.max(s, axis=1, keepdims=True))
            p = jnp.exp2((s - m_new[:, :1]) * SCORE_SCALE).astype(jnp.bfloat16)
            fade = jnp.exp2((m_old - m_new) * SCORE_SCALE)
            pv = jnp.dot(p, v, preferred_element_type=jnp.float32)
            acc_ref[at, :HEAD] = acc_ref[at, :HEAD] * fade + pv[:, :HEAD]
            acc_ref[at, HEAD:] = acc_ref[at, HEAD:] * fade + pv[:, HEAD:]
            m_ref[at, :] = m_new

    @pl.when(i == steps - 1)
    def _():
        for h in range(2):
            at = pl.ds(h * rows, rows)
            o_ref[:, h * HEAD : (h + 1) * HEAD] = (acc_ref[at, :HEAD] / acc_ref[at, HEAD:]).astype(jnp.bfloat16)


def flash(q, kv):
    keys, sub = 1536, 128
    steps = kv.shape[0] // keys
    rows = q.shape[0]
    return pl.pallas_call(
        functools.partial(flash_kernel, steps, sub),
        name="flash",
        grid=(steps,),
        in_specs=[
            pl.BlockSpec((rows, 2 * HEAD), lambda i: (0, 0)),
            pl.BlockSpec((keys, 2 * HEAD), lambda i: (i, 0)),
        ],
        out_specs=pl.BlockSpec((rows, 2 * HEAD), lambda i: (0, 0)),
        out_shape=jax.ShapeDtypeStruct((rows, 2 * HEAD), jnp.bfloat16),
        scratch_shapes=[
            pltpu.VMEM((2 * rows, HEAD), jnp.float32),
            pltpu.VMEM((2 * rows, 2 * HEAD), jnp.float32),
        ],
        compiler_params=pltpu.CompilerParams(vmem_limit_bytes=40 << 20),
        cost_estimate=pl.CostEstimate(flops=18_000_000_000, bytes_accessed=9_000_000, transcendentals=17_000_000),
    )(q, kv)


def body(
    latents, context, cond, ctx_cond, mod_weight, query_weight, key_matrix, value_matrix,
    out_weight, query_gain, key_gain,
):
    q, kv, gate = front(
        latents, context, cond, ctx_cond, mod_weight, query_weight, key_matrix, value_matrix,
        query_gain, key_gain,
    )
    attended = flash(q, lax.all_gather(kv, SP, axis=0, tiled=True))
    rows = lax.all_to_all(attended, TP, split_axis=0, concat_axis=1, tiled=True)
    weight = lax.all_gather(out_weight, TP, axis=0, tiled=True)
    mixed = jnp.dot(rows, weight, preferred_element_type=jnp.float32)
    mixed = mixed * lax.rsqrt(jnp.mean(mixed * mixed, axis=-1, keepdims=True) + NORM_EPS)
    return (latents.astype(jnp.float32) + gate * mixed).astype(jnp.bfloat16)


def solution(mesh):
    torus = Mesh(mesh.devices.reshape(Z, X, Y, C), AXES)
    placed = (
        P(AXES, None), P(SP, None), P(SP), P(SP), P(SP, TP), P(None, TP), P(None, TP), P(None, TP),
        P(TP, None), P(), P(),
    )
    return jax.shard_map(body, mesh=torus, in_specs=placed, out_specs=P(AXES, None), check_vma=False)
```

```python
import functools
import math

import jax
import jax.numpy as jnp
import numpy as np
from jax import lax
from jax.experimental import pallas as pl
from jax.experimental.pallas import tpu as pltpu
from jax.sharding import Mesh
from jax.sharding import PartitionSpec as P

GRID_W = 64
NORM_EPS = 1e-06
ROPE_BASE = 10000.0
Z, X, Y, C = 8, 4, 4, 2
AXES = ("z", "x", "y", "c")
SP = ("z", "x")
TP = ("y", "c")
MESH = pl.DeviceIdType.MESH
D = 2048
HEAD = 128
ROWS = 64
CTX_ROWS = 16
GROUP_ROWS = ROWS * Y * C
UNIT = CTX_ROWS + GROUP_ROWS
TOTAL_KEYS = UNIT * Z * X
LIFT = 16.0
SCORE_SCALE = HEAD ** (-0.5) * math.log2(math.e)


def coords():
    return tuple(lax.axis_index(a) for a in AXES)


def remote(src, dst, send, recv, dev):
    return pltpu.make_async_remote_copy(
        src_ref=src, dst_ref=dst, send_sem=send, recv_sem=recv, device_id=dev, device_id_type=MESH
    )


def meet(peers):
    barrier = pltpu.get_barrier_semaphore()
    for dev in peers:
        pl.semaphore_signal(barrier, inc=1, device_id=dev, device_id_type=MESH)
    pl.semaphore_wait(barrier, len(peers))


def rope_tables():
    quarter = HEAD // 4
    freq = (np.float32(ROPE_BASE) ** (-np.arange(quarter, dtype=np.float32) / np.float32(quarter))).astype(np.float32)
    lanes = freq[np.arange(HEAD) % quarter]
    sign = np.where(np.arange(HEAD) % (HEAD // 2) < quarter, -1.0, 1.0)
    grid_rows = GROUP_ROWS * Z * X // GRID_W
    row_angle = (np.arange(grid_rows, dtype=np.float32)[:, None] * lanes[None]).astype(np.float64)
    col_angle = (np.arange(GRID_W, dtype=np.float32)[:, None] * lanes[None]).astype(np.float64)
    as32 = lambda a: jnp.asarray(a.astype(np.float32))
    return (
        as32(np.cos(row_angle)),
        as32(np.sin(row_angle) * sign),
        as32(np.cos(col_angle)),
        as32(np.sin(col_angle) * sign),
    )


def column(row):
    n = row.shape[1]
    eye = lax.broadcasted_iota(jnp.int32, (n, n), 0) == lax.broadcasted_iota(jnp.int32, (n, n), 1)
    return jnp.sum(jnp.where(eye, row, 0.0), axis=1, keepdims=True)


def front_kernel(
    lat, ctx, cond, ctx_cond, modw, wq, wk, wv, q_gain, k_gain, cos_r, sin_r, cos_c, sin_c,
    q_out, kv_out, gate_out,
    xg, ws, cr, sr, part, x_in, x_sum, z_in, mod, xn, proj,
    w_sem, lat_send, lat_recv, x_send, x_recv, z_send, z_recv, t_send, t_recv,
):
    z, x, y, c = coords()
    me = y * C + c
    sp = z * X + x
    up, down = lax.rem(y + 1, Y), lax.rem(y + Y - 1, Y)
    far = lax.rem(y + 2, Y)
    loads = [
        pltpu.make_async_copy(wq, ws.at[:, pl.ds(0, 2 * HEAD)], w_sem.at[0]),
        pltpu.make_async_copy(wk, ws.at[:, pl.ds(2 * HEAD, HEAD)], w_sem.at[1]),
        pltpu.make_async_copy(wv, ws.at[:, pl.ds(3 * HEAD, HEAD)], w_sem.at[2]),
        pltpu.make_async_copy(cos_r.at[pl.ds(sp * 8, 8)], cr, w_sem.at[3]),
        pltpu.make_async_copy(sin_r.at[pl.ds(sp * 8, 8)], sr, w_sem.at[4]),
    ]
    for copy in loads:
        copy.start()
    x_peers = [(z, lax.rem(x + r, X), y, c) for r in range(1, X)]
    z_peers = [(lax.rem(z + r, Z), x, y, c) for r in range(1, Z)]
    t_rel = [(ry, rc) for ry in range(Y) for rc in range(C) if (ry, rc) != (0, 0)]
    t_peers = [(z, x, lax.rem(y + ry, Y), c + rc * (1 - 2 * c)) for ry, rc in t_rel]
    sib = (z, x, y, 1 - c)
    meet(x_peers + z_peers + t_peers)

    def slot(yy, cc):
        return yy * C + cc

    sends = []

    def send_lat(i, src, yy, cc, dev, lo=0, n=ROWS):
        copy = remote(src, xg.at[slot(yy, cc), pl.ds(lo, n)], lat_send.at[i], lat_recv.at[i], dev)
        copy.start()
        sends.append(copy)
        return copy

    up_dev, down_dev = (z, x, up, c), (z, x, down, c)
    c0 = send_lat(0, lat, y, c, up_dev)
    c1 = send_lat(1, lat, y, c, down_dev)
    c2 = send_lat(2, lat, y, c, sib)

    w = modw[...]
    for r, vec in enumerate((cond, ctx_cond)):
        v = vec[...]
        v = column(v * lax.logistic(v))
        row = jnp.sum(v * w, axis=0, keepdims=True)
        for i in range(6):
            part[r * 6 + i : r * 6 + i + 1, :] = row[:, i * HEAD : (i + 1) * HEAD]
    part[12:16, :] = jnp.zeros((4, HEAD), jnp.float32)
    xg[me] = lat[...]

    xs = [remote(part, x_in.at[i], x_send.at[i], x_recv.at[i], d) for i, d in enumerate(x_peers)]
    for s in xs:
        s.start()
    for s in xs:
        s.wait_recv()
    x_sum[...] = part[...] + x_in[0] + x_in[1] + x_in[2]
    zs = [remote(x_sum, z_in.at[i], z_send.at[i], z_recv.at[i], d) for i, d in enumerate(z_peers)]
    for s in zs:
        s.start()

    half = ROWS // 2
    c0.wait_recv()
    c3 = send_lat(3, xg.at[slot(down, c), pl.ds(0, half)], down, c, up_dev, 0, half)
    c5 = send_lat(5, xg.at[slot(down, c)], down, c, sib)
    c1.wait_recv()
    c4 = send_lat(4, xg.at[slot(up, c), pl.ds(half, half)], up, c, down_dev, half, half)
    c6 = send_lat(6, xg.at[slot(up, c)], up, c, sib)

    for s in zs:
        s.wait_recv()
    total = x_sum[...]
    for i in range(Z - 1):
        total = total + z_in[i]
    mod[me] = total
    ts = [remote(mod.at[me], mod.at[me], t_send.at[i], t_recv.at[i], d) for i, d in enumerate(t_peers)]
    for s in ts:
        s.start()
    c3.wait_recv()
    c4.wait_recv()
    c7 = send_lat(7, xg.at[slot(far, c)], far, c, sib)
    for copy in loads:
        copy.wait()
    for s in ts:
        s.wait_recv()

    def mod_row(r, first):
        tiles = [first + t for t in range(D // HEAD)]
        return jnp.concatenate([mod[t // 6, r * 6 + t % 6 : r * 6 + t % 6 + 1, :] for t in tiles], axis=1)

    gate_out[...] = mod_row(0, 32)

    def modulated(rows, r):
        v = rows.astype(jnp.float32)
        v = v * lax.rsqrt(jnp.mean(v * v, axis=-1, keepdims=True) + NORM_EPS)
        return (v * (1.0 + mod_row(r, 16)) + mod_row(r, 0)).astype(jnp.bfloat16)

    xn[:CTX_ROWS, :] = modulated(ctx[...], 1)
    for s in (c2, c5, c6, c7):
        s.wait_recv()
    for j in range(Y * C):
        xn[CTX_ROWS + ROWS * j : CTX_ROWS + ROWS * (j + 1), :] = modulated(xg[j], 0)

    lane = lax.broadcasted_iota(jnp.int32, (GRID_W, HEAD), 1)
    is_row = lane < HEAD // 2
    is_first = lax.rem(lane, HEAD // 2) < HEAD // 4

    def unit_rows(v, gain):
        return v * lax.rsqrt(jnp.mean(v * v, axis=-1, keepdims=True) + NORM_EPS) * gain

    for lo, n in ((0, UNIT // 2 + 8), (UNIT // 2 + 8, UNIT // 2 - 8)):
        proj[lo : lo + n, :] = jnp.dot(xn[lo : lo + n, :], ws[...], preferred_element_type=jnp.float32)
    qg, kg = q_gain[...], k_gain[...]
    kv_out[:CTX_ROWS, :HEAD] = unit_rows(proj[:CTX_ROWS, 2 * HEAD : 3 * HEAD], kg).astype(jnp.bfloat16)
    kv_out[:CTX_ROWS, HEAD:] = proj[:CTX_ROWS, 3 * HEAD :].astype(jnp.bfloat16) * jnp.bfloat16(LIFT)
    for j in range(GROUP_ROWS // GRID_W):
        lo = CTX_ROWS + GRID_W * j
        cos = jnp.where(is_row, cr[j : j + 1, :], cos_c[...])
        sin = jnp.where(is_row, sr[j : j + 1, :], sin_c[...])

        def turned(v, gain):
            v = unit_rows(v, gain)
            other = jnp.where(is_first, pltpu.roll(v, HEAD - HEAD // 4, 1), pltpu.roll(v, HEAD // 4, 1))
            return (v * cos + other * sin).astype(jnp.bfloat16)

        for h in range(2):
            q_out[GRID_W * j : GRID_W * (j + 1), h * HEAD : (h + 1) * HEAD] = turned(
                proj[lo : lo + GRID_W, h * HEAD : (h + 1) * HEAD], qg
            )
        kv_out[lo : lo + GRID_W, :HEAD] = turned(proj[lo : lo + GRID_W, 2 * HEAD : 3 * HEAD], kg)
        kv_out[lo : lo + GRID_W, HEAD:] = proj[lo : lo + GRID_W, 3 * HEAD :].astype(jnp.bfloat16)

    for s in sends + xs + zs + ts:
        s.wait_send()


def front(latents, context, cond, ctx_cond, mod_weight, wq, wk, wv, q_gain, k_gain):
    vm = pl.BlockSpec(memory_space=pltpu.VMEM)
    hbm = pl.BlockSpec(memory_space=pl.ANY)
    cos_r, sin_r, cos_c, sin_c = rope_tables()
    bf, f32 = jnp.bfloat16, jnp.float32
    dma = pltpu.SemaphoreType.DMA
    return pl.pallas_call(
        front_kernel,
        name="front",
        out_shape=(
            jax.ShapeDtypeStruct((GROUP_ROWS, 2 * HEAD), bf),
            jax.ShapeDtypeStruct((UNIT, 2 * HEAD), bf),
            jax.ShapeDtypeStruct((1, D), f32),
        ),
        in_specs=[vm] * 5 + [hbm] * 3 + [vm] * 2 + [hbm] * 2 + [vm] * 2,
        out_specs=(vm, vm, vm),
        scratch_shapes=[
            pltpu.VMEM((Y * C, ROWS, D), bf),
            pltpu.VMEM((D, 4 * HEAD), bf),
            pltpu.VMEM((8, HEAD), f32),
            pltpu.VMEM((8, HEAD), f32),
            pltpu.VMEM((16, HEAD), f32),
            pltpu.VMEM((X - 1, 16, HEAD), f32),
            pltpu.VMEM((16, HEAD), f32),
            pltpu.VMEM((Z - 1, 16, HEAD), f32),
            pltpu.VMEM((Y * C, 16, HEAD), f32),
            pltpu.VMEM((UNIT, D), bf),
            pltpu.VMEM((UNIT, 4 * HEAD), f32),
            dma((5,)), dma((8,)), dma((8,)), dma((X - 1,)), dma((X - 1,)),
            dma((Z - 1,)), dma((Z - 1,)), dma((7,)), dma((7,)),
        ],
        compiler_params=pltpu.CompilerParams(collective_id=0, has_side_effects=True, vmem_limit_bytes=40 << 20),
    )(
        latents, context, cond.reshape(1, -1), ctx_cond.reshape(1, -1), mod_weight, wq, wk, wv,
        q_gain.reshape(1, -1), k_gain.reshape(1, -1), cos_r, sin_r, cos_c, sin_c,
    )


H1 = 240
H2 = UNIT - H1
CHUNK = 1408
CHUNKS = TOTAL_KEYS // CHUNK
SUB = 128


def unit_order():
    order = [(0, "own", s) for s in (0, 1)] + [(0, "nbr", s) for s in (0, 1)]
    for t, col in ((1, "own"), (2, "own"), (1, "nbr"), (3, "own"), (2, "nbr"), (4, "own"), (3, "nbr"), (4, "nbr")):
        for s in (0, 1):
            order += [(d, col, s) for d in ((t, -t) if t < 4 else (4,))]
    return {u: i for i, u in enumerate(order)}


ORDER = unit_order()
DS = (0, 1, -1, 2, -2, 3, -3, 4)
KINDS = ("own", "nbr", "h2")


def main_kernel(
    q_in, kv_in, ow_in, lat_in, gate_in, out,
    keys, qb, ones, m_ref, acc, att, got, ow, lat, gate, mixed,
    loc, z_send, z_recv, x_send, x_recv, d_send, d_recv, o_send, o_recv, s_send, s_recv, a_send, a_recv,
):
    z, x, y, c = coords()
    me = y * C + c
    pair = x + 1 - 2 * lax.rem(x, 2)
    is_a = lax.rem((x + 1) // 2, 2)
    swapped = is_a == c
    row_x = x + (pair - x) * (1 - lax.rem(is_a + c, 2))
    head = y * C + 1 - is_a
    up, down, far = lax.rem(y + 1, Y), lax.rem(y + Y - 1, Y), lax.rem(y + 2, Y)
    sib = (z, x, y, 1 - c)
    partner = (z, pair, y, 1 - c)
    nbr = (z, X - 1 - x, y, c)
    z_up, z_down = (lax.rem(z + 1, Z), x, y, c), (lax.rem(z + Z - 1, Z), x, y, c)
    y_up, y_down = (z, x, up, c), (z, x, down, c)
    rel = [(ry, rc) for ry in range(Y) for rc in range(C)]
    flip = 1 - 2 * c

    local = [
        pltpu.make_async_copy(lat_in, lat, loc.at[2]),
        pltpu.make_async_copy(gate_in, gate, loc.at[3]),
        pltpu.make_async_copy(ow_in, ow.at[me], loc.at[4]),
    ]
    for copy in local:
        copy.start()
    q_local = pltpu.make_async_copy(q_in, qb, loc.at[0])
    kv_local = pltpu.make_async_copy(kv_in, keys.at[pl.ds(0, UNIT)], loc.at[1])

    @pl.when(jnp.logical_not(swapped))
    def _():
        kv_local.start()
        q_local.start()

    meet(
        [(z, x, lax.rem(y + ry, Y), c + rc * flip) for ry, rc in rel[1:]]
        + [(z, pair, lax.rem(y + ry, Y), c + rc * flip) for ry, rc in rel]
        + [z_up, z_down, nbr]
    )

    def at(d, col, s, lo, n):
        return keys.at[pl.ds(ORDER[(d, col, s)] * UNIT + lo, n)]

    def swap_kv():
        return remote(kv_in, keys.at[pl.ds(0, UNIT)], s_send.at[0], s_recv.at[0], partner)

    def swap_q():
        return remote(q_in, qb, s_send.at[1], s_recv.at[1], partner)

    def ring(direction, t, kind):
        col = "nbr" if kind == "nbr" else "own"
        lo, n = (H1, H2) if kind == "h2" else (0, H1)
        if kind == "h2" and t == 4:
            n = H2 // 2
            lo = lo if direction > 0 else lo + n
        dst = 4 if t == 4 else direction * t
        i = (0 if direction > 0 else 12) + (t - 1) * 3 + KINDS.index(kind)
        return remote(
            at(direction * (t - 1), col, 0, lo, n), at(dst, col, 0, lo, n), z_send.at[i], z_recv.at[i],
            z_up if direction > 0 else z_down,
        )

    def used(direction, t, kind):
        return t < 4 or kind == "h2" or (kind == "own") == (direction > 0)

    def cross(d):
        i = DS.index(d)
        return remote(at(d, "own", 0, H1, H2), at(d, "nbr", 0, H1, H2), x_send.at[i], x_recv.at[i], nbr)

    def cross_h1():
        return remote(at(0, "own", 0, 0, H1), at(0, "nbr", 0, 0, H1), x_send.at[8], x_recv.at[8], nbr)

    def share(d, col):
        i = DS.index(d) + (0 if col == "own" else 8)
        return remote(at(d, col, 0, 0, UNIT), at(d, col, 1, 0, UNIT), d_send.at[i], d_recv.at[i], sib)

    half = 2 * HEAD // 2

    def weight(i):
        who = [
            (ow_in, me, 0, 2 * half, y_up), (ow_in, me, 0, 2 * half, y_down), (ow_in, me, 0, 2 * half, sib),
            (None, down * C + c, 0, half, y_up), (None, up * C + c, half, half, y_down),
            (None, down * C + c, 0, 2 * half, sib), (None, up * C + c, 0, 2 * half, sib),
            (None, far * C + c, 0, 2 * half, sib),
        ][i]
        src, slot, lo, n, dev = who
        dst = ow.at[slot, pl.ds(lo, n)]
        return remote(dst if src is None else src, dst, o_send.at[i], o_recv.at[i], dev)

    def on_ring(t, kind):
        for direction in (1, -1):
            if used(direction, t, kind):
                ring(direction, t, kind).wait_recv()
            if t < 4 and used(direction, t + 1, kind):
                ring(direction, t + 1, kind).start()

    def begin():
        for i in range(3):
            weight(i).start()

        @pl.when(swapped)
        def _():
            swap_kv().start()
            swap_q().start()
            swap_kv().wait_recv()

        @pl.when(jnp.logical_not(swapped))
        def _():
            kv_local.wait()

        cross_h1().start()
        for kind in ("own", "h2"):
            for direction in (1, -1):
                ring(direction, 1, kind).start()
        share(0, "own").start()
        cross(0).start()

    def own_done(t):
        on_ring(t, "h2")
        for d in ((t, -t) if t < 4 else (4,)):
            cross(d).start()
            share(d, "own").start()

    def nbr_done(t):
        for d in ((t, -t) if 0 < t < 4 else (t,)):
            cross(d).wait_recv()
            share(d, "nbr").start()

    def shared(t, col):
        for d in ((t, -t) if 0 < t < 4 else (t,)):
            share(d, col).wait_recv()

    def step0():
        cross_h1().wait_recv()
        for direction in (1, -1):
            ring(direction, 1, "nbr").start()
        on_ring(1, "own")
        nbr_done(0)
        own_done(1)

        @pl.when(swapped)
        def _():
            swap_q().wait_recv()

        @pl.when(jnp.logical_not(swapped))
        def _():
            q_local.wait()

        shared(0, "own")

    def step1():
        shared(0, "nbr")
        on_ring(1, "nbr")

    def step2():
        shared(1, "own")
        on_ring(2, "own")

    def step3():
        own_done(2)
        shared(2, "own")

    def step4():
        nbr_done(1)
        on_ring(2, "nbr")

    def step5():
        shared(1, "nbr")
        on_ring(3, "own")

    def step6():
        own_done(3)
        shared(3, "own")

    def step7():
        nbr_done(2)
        on_ring(3, "nbr")
        for i in (0, 1):
            weight(i).wait_recv()
        for i in (3, 4, 5, 6):
            weight(i).start()

    def step8():
        shared(2, "nbr")

    def step9():
        on_ring(4, "own")
        own_done(4)
        nbr_done(3)
        shared(4, "own")

    def step10():
        shared(3, "nbr")

    def step11():
        on_ring(4, "nbr")
        nbr_done(4)
        shared(4, "nbr")

    steps = (step0, step1, step2, step3, step4, step5, step6, step7, step8, step9, step10, step11)

    begin()
    ones[...] = jnp.ones_like(ones)
    for u in range(3 * CHUNK // UNIT):
        ones[UNIT * u : UNIT * u + CTX_ROWS, :] = jnp.full((CTX_ROWS, HEAD), LIFT, jnp.bfloat16)
    m_ref[...] = jnp.full_like(m_ref, -1e30)
    acc[...] = jnp.zeros_like(acc)

    def chunk(i, carry):
        for j, step in enumerate(steps):
            pl.when(i == j)(step)
        rows = pl.ds(pl.multiple_of(i * CHUNK, CHUNK), CHUNK)
        k = keys[rows, :HEAD]
        w = ones[pl.ds(pl.multiple_of(lax.rem(i, 3) * CHUNK, CHUNK), CHUNK), :]
        v = jnp.concatenate([keys[rows, HEAD:], w], axis=1)
        for h in range(2):
            for r in range(0, GROUP_ROWS, SUB):
                sl = pl.ds(h * GROUP_ROWS + r, SUB)
                s = lax.dot_general(
                    qb[r : r + SUB, h * HEAD : (h + 1) * HEAD], k, (((1,), (1,)), ((), ())),
                    preferred_element_type=jnp.float32,
                )
                m_old = m_ref[sl, :]
                m_new = jnp.maximum(m_old, jnp.max(s, axis=1, keepdims=True))
                p = jnp.exp2((s - m_new[:, :1]) * SCORE_SCALE).astype(jnp.bfloat16)
                fade = jnp.exp2((m_old - m_new) * SCORE_SCALE)
                pv = jnp.dot(p, v, preferred_element_type=jnp.float32)
                acc[sl, :HEAD] = acc[sl, :HEAD] * fade + pv[:, :HEAD]
                acc[sl, HEAD:] = acc[sl, HEAD:] * fade + pv[:, HEAD:]
                m_ref[sl, :] = m_new
        return carry

    lax.fori_loop(0, CHUNKS, chunk, 0)

    for i in (3, 4):
        weight(i).wait_recv()
    weight(7).start()
    for h in range(2):
        sl = pl.ds(h * GROUP_ROWS, GROUP_ROWS)
        att[:, h * HEAD : (h + 1) * HEAD] = (acc[sl, :HEAD] / acc[sl, HEAD:]).astype(jnp.bfloat16)

    def hand(i):
        ry, rc = rel[i]
        yy, cc = lax.rem(y + ry, Y), c + rc * flip
        src = att.at[pl.ds(pl.multiple_of((yy * C + cc) * ROWS, ROWS), ROWS)]
        return remote(src, got.at[head], a_send.at[i], a_recv.at[head], (z, row_x, yy, cc))

    for i in range(1, Y * C):
        hand(i).start()

    @pl.when(swapped)
    def _():
        hand(0).start()

    @pl.when(jnp.logical_not(swapped))
    def _():
        got[head] = att[pl.ds(pl.multiple_of(me * ROWS, ROWS), ROWS), :]

    for copy in local:
        copy.wait()
    for i in (2, 5, 6, 7):
        weight(i).wait_recv()
    for j in range(Y * C):

        @pl.when(jnp.logical_or(swapped, head != j))
        def _():
            remote(att.at[pl.ds(0, ROWS)], got.at[j], a_send.at[0], a_recv.at[j], sib).wait_recv()

    rows = jnp.concatenate([got[j] for j in range(Y * C)], axis=1)
    for n in range(0, D, 512):
        total = jnp.zeros((ROWS, 512), jnp.float32)
        for j in range(Y * C):
            total = total + jnp.dot(
                rows[:, j * 2 * HEAD : (j + 1) * 2 * HEAD], ow[j, :, n : n + 512], preferred_element_type=jnp.float32
            )
        mixed[:, n : n + 512] = total
    v = mixed[...]
    v = v * lax.rsqrt(jnp.mean(v * v, axis=-1, keepdims=True) + NORM_EPS)
    out[...] = (lat[...].astype(jnp.float32) + gate[...] * v).astype(jnp.bfloat16)

    for kind in KINDS:
        for t in range(1, 5):
            for direction in (1, -1):
                if used(direction, t, kind):
                    ring(direction, t, kind).wait_send()
    for d in DS:
        cross(d).wait_send()
        share(d, "own").wait_send()
        share(d, "nbr").wait_send()
    cross_h1().wait_send()
    for i in range(8):
        weight(i).wait_send()
    for i in range(1, Y * C):
        hand(i).wait_send()

    @pl.when(swapped)
    def _():
        hand(0).wait_send()
        swap_kv().wait_send()
        swap_q().wait_send()


def attend(q, kv, out_weight, latents, gate):
    hbm = pl.BlockSpec(memory_space=pltpu.HBM)
    bf, f32 = jnp.bfloat16, jnp.float32
    dma = pltpu.SemaphoreType.DMA
    return pl.pallas_call(
        main_kernel,
        name="attend",
        out_shape=jax.ShapeDtypeStruct((ROWS, D), bf),
        in_specs=[hbm] * 5,
        out_specs=pl.BlockSpec(memory_space=pltpu.VMEM),
        scratch_shapes=[
            pltpu.VMEM((TOTAL_KEYS, 2 * HEAD), bf),
            pltpu.VMEM((GROUP_ROWS, 2 * HEAD), bf),
            pltpu.VMEM((3 * CHUNK, HEAD), bf),
            pltpu.VMEM((2 * GROUP_ROWS, HEAD), f32),
            pltpu.VMEM((2 * GROUP_ROWS, 2 * HEAD), f32),
            pltpu.VMEM((GROUP_ROWS, 2 * HEAD), bf),
            pltpu.VMEM((Y * C, ROWS, 2 * HEAD), bf),
            pltpu.VMEM((Y * C, 2 * HEAD, D), bf),
            pltpu.VMEM((ROWS, D), bf),
            pltpu.VMEM((1, D), f32),
            pltpu.VMEM((ROWS, D), f32),
            dma((5,)), dma((24,)), dma((24,)), dma((9,)), dma((9,)), dma((16,)), dma((16,)),
            dma((8,)), dma((8,)), dma((2,)), dma((2,)), dma((8,)), dma((8,)),
        ],
        compiler_params=pltpu.CompilerParams(collective_id=1, has_side_effects=True, vmem_limit_bytes=60 << 20),
    )(q, kv, out_weight, latents, gate)


def body(
    latents, context, cond, ctx_cond, mod_weight, query_weight, key_matrix, value_matrix,
    out_weight, query_gain, key_gain,
):
    q, kv, gate = front(
        latents, context, cond, ctx_cond, mod_weight, query_weight, key_matrix, value_matrix,
        query_gain, key_gain,
    )
    return attend(q, kv, out_weight, latents, gate)


def solution(mesh):
    torus = Mesh(mesh.devices.reshape(Z, X, Y, C), AXES)
    placed = (
        P(AXES, None), P(SP, None), P(SP), P(SP), P(SP, TP), P(None, TP), P(None, TP), P(None, TP),
        P(TP, None), P(), P(),
    )
    return jax.shard_map(body, mesh=torus, in_specs=placed, out_specs=P(AXES, None), check_vma=False)
```

```python
import functools
import math

import jax
import jax.numpy as jnp
import numpy as np
from jax import lax
from jax.experimental import pallas as pl
from jax.experimental.pallas import tpu as pltpu
from jax.sharding import Mesh
from jax.sharding import PartitionSpec as P

GRID_W = 64
NORM_EPS = 1e-06
ROPE_BASE = 10000.0
Z, X, Y, C = 8, 4, 4, 2
AXES = ("z", "x", "y", "c")
SP = ("z", "x")
TP = ("y", "c")
MESH = pl.DeviceIdType.MESH
D = 2048
HEAD = 128
ROWS = 64
CTX_ROWS = 16
GROUP_ROWS = ROWS * Y * C
UNIT = CTX_ROWS + GROUP_ROWS
TOTAL_KEYS = UNIT * Z * X
LIFT = 16.0
SCORE_SCALE = HEAD ** (-0.5) * math.log2(math.e)


def coords():
    return tuple(lax.axis_index(a) for a in AXES)


def remote(src, dst, send, recv, dev):
    return pltpu.make_async_remote_copy(
        src_ref=src, dst_ref=dst, send_sem=send, recv_sem=recv, device_id=dev, device_id_type=MESH
    )


def meet(peers):
    barrier = pltpu.get_barrier_semaphore()
    for dev in peers:
        pl.semaphore_signal(barrier, inc=1, device_id=dev, device_id_type=MESH)
    pl.semaphore_wait(barrier, len(peers))


def rope_tables():
    quarter = HEAD // 4
    freq = (np.float32(ROPE_BASE) ** (-np.arange(quarter, dtype=np.float32) / np.float32(quarter))).astype(np.float32)
    lanes = freq[np.arange(HEAD) % quarter]
    sign = np.where(np.arange(HEAD) % (HEAD // 2) < quarter, -1.0, 1.0)
    grid_rows = GROUP_ROWS * Z * X // GRID_W
    row_angle = (np.arange(grid_rows, dtype=np.float32)[:, None] * lanes[None]).astype(np.float64)
    col_angle = (np.arange(GRID_W, dtype=np.float32)[:, None] * lanes[None]).astype(np.float64)
    as32 = lambda a: jnp.asarray(a.astype(np.float32))
    return (
        as32(np.cos(row_angle)),
        as32(np.sin(row_angle) * sign),
        as32(np.cos(col_angle)),
        as32(np.sin(col_angle) * sign),
    )


def column(row):
    n = row.shape[1]
    eye = lax.broadcasted_iota(jnp.int32, (n, n), 0) == lax.broadcasted_iota(jnp.int32, (n, n), 1)
    return jnp.sum(jnp.where(eye, row, 0.0), axis=1, keepdims=True)


H1 = 240
H2 = UNIT - H1
CHUNK = 1408
CHUNKS = TOTAL_KEYS // CHUNK
SUB = 352


def unit_order():
    order = [(0, "own", s) for s in (0, 1)] + [(0, "nbr", s) for s in (0, 1)]
    for t, col in ((1, "own"), (2, "own"), (1, "nbr"), (3, "own"), (2, "nbr"), (4, "own"), (3, "nbr"), (4, "nbr")):
        for s in (0, 1):
            order += [(d, col, s) for d in ((t, -t) if t < 4 else (4,))]
    return {u: i for i, u in enumerate(order)}


ORDER = unit_order()
DS = (0, 1, -1, 2, -2, 3, -3, 4)
KINDS = ("own", "nbr", "h2")


def layer_kernel(
    lat_in, ctx_in, cond_in, ctx_cond_in, modw_in, wq, wk, wv, ow_in, q_gain_in, k_gain_in, cos_r, sin_r, cos_c_in, sin_c_in,
    out,
    lat, ctx, cond, ctx_cond, modw, q_gain, k_gain, cos_c, sin_c, cr, sr,
    xg, wqs, wkv, part, x_in, x_sum, z_in, mod, xn, kvb, qt,
    keys, qb, ones, m_ref, acc, att, got, ow, mixed,
    loc, lat_send, lat_recv, mx_send, mx_recv, mz_send, mz_recv, mt_send, mt_recv,
    z_send, z_recv, x_send, x_recv, d_send, d_recv, o_send, o_recv, s_send, s_recv, a_send, a_recv,
):
    z, x, y, c = coords()
    me = y * C + c
    sp = z * X + x
    pair = x + 1 - 2 * lax.rem(x, 2)
    is_a = lax.rem((x + 1) // 2, 2)
    swapped = is_a == c
    row_x = x + (pair - x) * (1 - lax.rem(is_a + c, 2))
    head = y * C + 1 - is_a
    up, down, far = lax.rem(y + 1, Y), lax.rem(y + Y - 1, Y), lax.rem(y + 2, Y)
    sib = (z, x, y, 1 - c)
    partner = (z, pair, y, 1 - c)
    nbr = (z, X - 1 - x, y, c)
    z_up, z_down = (lax.rem(z + 1, Z), x, y, c), (lax.rem(z + Z - 1, Z), x, y, c)
    y_up, y_down = (z, x, up, c), (z, x, down, c)
    rel = [(ry, rc) for ry in range(Y) for rc in range(C)]
    flip = 1 - 2 * c
    x_peers = [(z, lax.rem(x + r, X), y, c) for r in range(1, X)]
    z_peers = [(lax.rem(z + r, Z), x, y, c) for r in range(1, Z)]
    t_peers = [(z, x, lax.rem(y + ry, Y), c + rc * flip) for ry, rc in rel[1:]]

    loads = [
        pltpu.make_async_copy(src, dst, loc.at[i])
        for i, (src, dst) in enumerate((
            (modw_in, modw), (cond_in, cond), (ctx_cond_in, ctx_cond), (lat_in, lat), (ctx_in, ctx),
            (q_gain_in, q_gain), (k_gain_in, k_gain), (cos_c_in, cos_c), (sin_c_in, sin_c),
            (cos_r.at[pl.ds(sp * 8, 8)], cr), (sin_r.at[pl.ds(sp * 8, 8)], sr),
            (wk, wkv.at[:, pl.ds(0, HEAD)]), (wv, wkv.at[:, pl.ds(HEAD, HEAD)]), (wq, wqs), (ow_in, ow.at[me]),
        ))
    ]
    for copy in loads:
        copy.start()
    meet(x_peers + z_peers + t_peers + [(z, pair, lax.rem(y + ry, Y), c + rc * flip) for ry, rc in rel[1:]])

    lat_sends = []

    def send_lat(i, src, yy, dev, lo=0, n=ROWS):
        copy = remote(src, xg.at[yy * C + c, pl.ds(lo, n)], lat_send.at[i], lat_recv.at[i], dev)
        copy.start()
        lat_sends.append(copy)
        return copy

    c0 = send_lat(0, lat_in, y, y_up)
    c1 = send_lat(1, lat_in, y, y_down)
    c2 = send_lat(2, lat_in, y, sib)
    for copy in loads[:5]:
        copy.wait()

    w = modw[...]
    for r, vec in enumerate((cond, ctx_cond)):
        v = vec[...]
        v = column(v * lax.logistic(v))
        row = jnp.sum(v * w, axis=0, keepdims=True)
        for i in range(6):
            part[r * 6 + i : r * 6 + i + 1, :] = row[:, i * HEAD : (i + 1) * HEAD]
    part[12:16, :] = jnp.zeros((4, HEAD), jnp.float32)

    xs = [remote(part, x_in.at[i], mx_send.at[i], mx_recv.at[i], d) for i, d in enumerate(x_peers)]
    for s in xs:
        s.start()
    xg[me] = lat[...]
    wt = lax.broadcasted_iota(jnp.int32, ones.shape, 1)
    ones[...] = jnp.where(lax.rem(wt, UNIT) < CTX_ROWS, LIFT, 1.0).astype(jnp.bfloat16)
    m_ref[...] = jnp.full_like(m_ref, -1e30)
    acc[...] = jnp.zeros_like(acc)
    for s in xs:
        s.wait_recv()
    x_sum[...] = part[...] + x_in[0] + x_in[1] + x_in[2]
    zs = [remote(x_sum, z_in.at[i], mz_send.at[i], mz_recv.at[i], d) for i, d in enumerate(z_peers)]
    for s in zs:
        s.start()

    hr = ROWS // 2
    c0.wait_recv()
    c3 = send_lat(3, xg.at[down * C + c, pl.ds(0, hr)], down, y_up, 0, hr)
    c5 = send_lat(5, xg.at[down * C + c], down, sib)
    c1.wait_recv()
    c4 = send_lat(4, xg.at[up * C + c, pl.ds(hr, hr)], up, y_down, hr, hr)
    c6 = send_lat(6, xg.at[up * C + c], up, sib)

    for s in zs:
        s.wait_recv()
    total = x_sum[...]
    for i in range(Z - 1):
        total = total + z_in[i]
    mod[me] = total
    ts = [remote(mod.at[me], mod.at[me], mt_send.at[i], mt_recv.at[i], d) for i, d in enumerate(t_peers)]
    for s in ts:
        s.start()
    for copy in loads[5:]:
        copy.wait()
    for s in ts:
        s.wait_recv()

    def mod_row(r, first):
        tiles = [first + t for t in range(D // HEAD)]
        return jnp.concatenate([mod[t // 6, r * 6 + t % 6 : r * 6 + t % 6 + 1, :] for t in tiles], axis=1)

    def modulated(rows, r):
        v = rows.astype(jnp.float32)
        v = v * lax.rsqrt(jnp.mean(v * v, axis=-1, keepdims=True) + NORM_EPS)
        return (v * (1.0 + mod_row(r, 16)) + mod_row(r, 0)).astype(jnp.bfloat16)

    def make_rows(j):
        lo = pl.multiple_of(CTX_ROWS + ROWS * j, CTX_ROWS)
        xn[pl.ds(lo, ROWS), :] = modulated(xg[j], 0)

    xn[:CTX_ROWS, :] = modulated(ctx[...], 1)
    make_rows(me)
    c2.wait_recv()
    make_rows(y * C + 1 - c)
    make_rows(down * C + c)
    make_rows(up * C + c)
    c3.wait_recv()
    c4.wait_recv()
    c7 = send_lat(7, xg.at[far * C + c], far, sib)
    make_rows(far * C + c)
    c5.wait_recv()
    make_rows(down * C + 1 - c)
    c6.wait_recv()
    make_rows(up * C + 1 - c)
    c7.wait_recv()
    make_rows(far * C + 1 - c)

    lane = lax.broadcasted_iota(jnp.int32, (GRID_W, HEAD), 1)
    is_row = lane < HEAD // 2
    is_first = lax.rem(lane, HEAD // 2) < HEAD // 4

    def unit_rows(v, gain):
        return v * lax.rsqrt(jnp.mean(v * v, axis=-1, keepdims=True) + NORM_EPS) * gain

    def turned(v, gain, j):
        cos = jnp.where(is_row, cr[j : j + 1, :], cos_c[...])
        sin = jnp.where(is_row, sr[j : j + 1, :], sin_c[...])
        v = unit_rows(v, gain)
        other = jnp.where(is_first, pltpu.roll(v, HEAD - HEAD // 4, 1), pltpu.roll(v, HEAD // 4, 1))
        return (v * cos + other * sin).astype(jnp.bfloat16)

    qg, kg = q_gain[...], k_gain[...]
    blocks = GROUP_ROWS // GRID_W

    def at(d, col, s, lo, n):
        return keys.at[pl.ds(ORDER[(d, col, s)] * UNIT + lo, n)]

    def swap_kv():
        return remote(kvb, keys.at[pl.ds(0, UNIT)], s_send.at[0], s_recv.at[0], partner)

    def swap_q():
        return remote(qt, qb, s_send.at[1], s_recv.at[1], partner)

    def ring(direction, t, kind):
        col = "nbr" if kind == "nbr" else "own"
        lo, n = (H1, H2) if kind == "h2" else (0, H1)
        if kind == "h2" and t == 4:
            n = H2 // 2
            lo = lo if direction > 0 else lo + n
        dst = 4 if t == 4 else direction * t
        i = (0 if direction > 0 else 12) + (t - 1) * 3 + KINDS.index(kind)
        return remote(
            at(direction * (t - 1), col, 0, lo, n), at(dst, col, 0, lo, n), z_send.at[i], z_recv.at[i],
            z_up if direction > 0 else z_down,
        )

    def used(direction, t, kind):
        return t < 4 or kind == "h2" or (kind == "own") == (direction > 0)

    def cross(d):
        i = DS.index(d)
        return remote(at(d, "own", 0, H1, H2), at(d, "nbr", 0, H1, H2), x_send.at[i], x_recv.at[i], nbr)

    def cross_h1():
        return remote(at(0, "own", 0, 0, H1), at(0, "nbr", 0, 0, H1), x_send.at[8], x_recv.at[8], nbr)

    def share(d, col):
        i = DS.index(d) + (0 if col == "own" else 8)
        return remote(at(d, col, 0, 0, UNIT), at(d, col, 1, 0, UNIT), d_send.at[i], d_recv.at[i], sib)

    half = 2 * HEAD // 2

    def weight(i):
        who = [
            (ow_in, me, 0, 2 * half, y_up), (ow_in, me, 0, 2 * half, y_down), (ow_in, me, 0, 2 * half, sib),
            (None, down * C + c, 0, half, y_up), (None, up * C + c, half, half, y_down),
            (None, down * C + c, 0, 2 * half, sib), (None, up * C + c, 0, 2 * half, sib),
            (None, far * C + c, 0, 2 * half, sib),
        ][i]
        src, slot, lo, n, dev = who
        dst = ow.at[slot, pl.ds(lo, n)]
        return remote(dst if src is None else src, dst, o_send.at[i], o_recv.at[i], dev)

    def on_ring(t, kind):
        for direction in (1, -1):
            if used(direction, t, kind):
                ring(direction, t, kind).wait_recv()
            if t < 4 and used(direction, t + 1, kind):
                ring(direction, t + 1, kind).start()


    for i in range(3):
        weight(i).start()
    proj = jnp.dot(xn[...], wkv[...], preferred_element_type=jnp.float32)
    kvb[:CTX_ROWS, :HEAD] = unit_rows(proj[:CTX_ROWS, :HEAD], kg).astype(jnp.bfloat16)
    kvb[:CTX_ROWS, HEAD:] = proj[:CTX_ROWS, HEAD:].astype(jnp.bfloat16) * jnp.bfloat16(LIFT)
    for j in range(blocks):
        lo = CTX_ROWS + GRID_W * j
        kvb[lo : lo + GRID_W, :HEAD] = turned(proj[lo : lo + GRID_W, :HEAD], kg, j)
        kvb[lo : lo + GRID_W, HEAD:] = proj[lo : lo + GRID_W, HEAD:].astype(jnp.bfloat16)

    @pl.when(swapped)
    def _():
        swap_kv().start()

    @pl.when(jnp.logical_not(swapped))
    def _():
        keys[:UNIT, :] = kvb[...]

    def launch():
        cross_h1().start()
        for kind in ("own", "h2"):
            for direction in (1, -1):
                ring(direction, 1, kind).start()
        share(0, "own").start()
        cross(0).start()

    @pl.when(jnp.logical_not(swapped))
    def _():
        launch()

    proj = jnp.dot(xn[CTX_ROWS:, :], wqs[...], preferred_element_type=jnp.float32)
    for j in range(blocks):
        lo = GRID_W * j
        for h in range(2):
            qt[h * GROUP_ROWS + lo : h * GROUP_ROWS + lo + GRID_W, :] = turned(
                proj[lo : lo + GRID_W, h * HEAD : (h + 1) * HEAD], qg, j
            )

    @pl.when(swapped)
    def _():
        swap_q().start()
        swap_kv().wait_recv()
        launch()

    @pl.when(jnp.logical_not(swapped))
    def _():
        qb[...] = qt[...]

    def own_done(t):
        on_ring(t, "h2")
        for d in ((t, -t) if t < 4 else (4,)):
            cross(d).start()
            share(d, "own").start()

    def nbr_done(t):
        for d in ((t, -t) if 0 < t < 4 else (t,)):
            cross(d).wait_recv()
            share(d, "nbr").start()

    def shared(t, col):
        for d in ((t, -t) if 0 < t < 4 else (t,)):
            share(d, col).wait_recv()

    def step0():
        cross_h1().wait_recv()
        for direction in (1, -1):
            ring(direction, 1, "nbr").start()
        on_ring(1, "own")
        nbr_done(0)
        own_done(1)

        @pl.when(swapped)
        def _():
            swap_q().wait_recv()

        shared(0, "own")

    def step1():
        shared(0, "nbr")
        on_ring(1, "nbr")

    def step2():
        shared(1, "own")
        on_ring(2, "own")

    def step3():
        own_done(2)
        shared(2, "own")

    def step4():
        for i in (0, 1):
            weight(i).wait_recv()
        for i in (3, 4, 5, 6):
            weight(i).start()
        nbr_done(1)
        on_ring(2, "nbr")

    def step5():
        shared(1, "nbr")
        on_ring(3, "own")

    def step6():
        own_done(3)
        shared(3, "own")

    def step7():
        nbr_done(2)
        on_ring(3, "nbr")

    def step8():
        shared(2, "nbr")

    def step9():
        on_ring(4, "own")
        own_done(4)
        nbr_done(3)
        shared(4, "own")

    def step10():
        for i in (3, 4):
            weight(i).wait_recv()
        weight(7).start()
        shared(3, "nbr")

    def step11():
        on_ring(4, "nbr")
        nbr_done(4)
        shared(4, "nbr")

    steps = (step0, step1, step2, step3, step4, step5, step6, step7, step8, step9, step10, step11)


    def chunk(i, carry):
        for j, step in enumerate(steps):
            pl.when(i == j)(step)
        rows = pl.ds(pl.multiple_of(i * CHUNK, CHUNK), CHUNK)
        k = keys[rows, :HEAD]
        q = qb[...]
        scores = [
            lax.dot_general(k[a : a + SUB], q, (((1,), (1,)), ((), ())), preferred_element_type=jnp.float32)
            for a in range(0, CHUNK, SUB)
        ]
        weights = ones[:, pl.ds(pl.multiple_of(lax.rem(i, 3) * CHUNK, HEAD), CHUNK)]
        v = jnp.concatenate([keys[rows, HEAD:].T, weights], axis=0)
        m_old = m_ref[0:1, :]
        m_new = m_old
        for s in scores:
            m_new = jnp.maximum(m_new, jnp.max(s, axis=0, keepdims=True))
        p = jnp.concatenate([jnp.exp2((s - m_new) * SCORE_SCALE).astype(jnp.bfloat16) for s in scores], axis=0)
        fade = jnp.exp2((m_old - m_new) * SCORE_SCALE)
        acc[...] = acc[...] * fade + jnp.dot(v, p, preferred_element_type=jnp.float32)
        m_ref[...] = jnp.broadcast_to(m_new, m_ref.shape)
        return carry

    lax.fori_loop(0, CHUNKS, chunk, 0)

    for h in range(2):
        sl = pl.ds(h * GROUP_ROWS, GROUP_ROWS)
        att[:, h * HEAD : (h + 1) * HEAD] = (acc[:HEAD, sl] / acc[HEAD : HEAD + 1, sl]).T.astype(jnp.bfloat16)

    def hand(i):
        ry, rc = rel[i]
        yy, cc = lax.rem(y + ry, Y), c + rc * flip
        src = att.at[pl.ds(pl.multiple_of((yy * C + cc) * ROWS, ROWS), ROWS)]
        return remote(src, got.at[head], a_send.at[i], a_recv.at[head], (z, row_x, yy, cc))

    for i in range(1, Y * C):
        hand(i).start()

    @pl.when(swapped)
    def _():
        hand(0).start()

    @pl.when(jnp.logical_not(swapped))
    def _():
        got[head] = att[pl.ds(pl.multiple_of(me * ROWS, ROWS), ROWS), :]

    for i in (2, 5, 6, 7):
        weight(i).wait_recv()
    for j in range(Y * C):

        @pl.when(jnp.logical_or(swapped, head != j))
        def _():
            remote(att.at[pl.ds(0, ROWS)], got.at[j], a_send.at[0], a_recv.at[j], sib).wait_recv()

    rows = jnp.concatenate([got[j] for j in range(Y * C)], axis=1)
    for n in range(0, D, 512):
        total = jnp.zeros((ROWS, 512), jnp.float32)
        for j in range(Y * C):
            total = total + jnp.dot(
                rows[:, j * 2 * HEAD : (j + 1) * 2 * HEAD], ow[j, :, n : n + 512], preferred_element_type=jnp.float32
            )
        mixed[:, n : n + 512] = total
    v = mixed[...]
    v = v * lax.rsqrt(jnp.mean(v * v, axis=-1, keepdims=True) + NORM_EPS)
    out[...] = (lat[...].astype(jnp.float32) + mod_row(0, 32) * v).astype(jnp.bfloat16)

    for kind in KINDS:
        for t in range(1, 5):
            for direction in (1, -1):
                if used(direction, t, kind):
                    ring(direction, t, kind).wait_send()
    for d in DS:
        cross(d).wait_send()
        share(d, "own").wait_send()
        share(d, "nbr").wait_send()
    cross_h1().wait_send()
    for i in range(8):
        weight(i).wait_send()
    for i in range(1, Y * C):
        hand(i).wait_send()


    for s in lat_sends + xs + zs + ts:
        s.wait_send()

    @pl.when(swapped)
    def _():
        hand(0).wait_send()
        swap_kv().wait_send()
        swap_q().wait_send()


def layer(latents, context, cond, ctx_cond, mod_weight, wq, wk, wv, out_weight, q_gain, k_gain):
    hbm = pl.BlockSpec(memory_space=pltpu.HBM)
    bf, f32 = jnp.bfloat16, jnp.float32
    dma = pltpu.SemaphoreType.DMA
    return pl.pallas_call(
        layer_kernel,
        name="layer",
        out_shape=jax.ShapeDtypeStruct((ROWS, D), bf),
        in_specs=[hbm] * 15,
        out_specs=pl.BlockSpec(memory_space=pltpu.VMEM),
        scratch_shapes=[
            pltpu.VMEM((ROWS, D), bf),
            pltpu.VMEM((CTX_ROWS, D), bf),
            pltpu.VMEM((1, ROWS), f32),
            pltpu.VMEM((1, ROWS), f32),
            pltpu.VMEM((ROWS, 6 * HEAD), f32),
            pltpu.VMEM((1, HEAD), f32),
            pltpu.VMEM((1, HEAD), f32),
            pltpu.VMEM((GRID_W, HEAD), f32),
            pltpu.VMEM((GRID_W, HEAD), f32),
            pltpu.VMEM((8, HEAD), f32),
            pltpu.VMEM((8, HEAD), f32),
            pltpu.VMEM((Y * C, ROWS, D), bf),
            pltpu.VMEM((D, 2 * HEAD), bf),
            pltpu.VMEM((D, 2 * HEAD), bf),
            pltpu.VMEM((16, HEAD), f32),
            pltpu.VMEM((X - 1, 16, HEAD), f32),
            pltpu.VMEM((16, HEAD), f32),
            pltpu.VMEM((Z - 1, 16, HEAD), f32),
            pltpu.VMEM((Y * C, 16, HEAD), f32),
            pltpu.VMEM((UNIT, D), bf),
            pltpu.VMEM((UNIT, 2 * HEAD), bf),
            pltpu.VMEM((2 * GROUP_ROWS, HEAD), bf),
            pltpu.VMEM((TOTAL_KEYS, 2 * HEAD), bf),
            pltpu.VMEM((2 * GROUP_ROWS, HEAD), bf),
            pltpu.VMEM((16, 3 * CHUNK), bf),
            pltpu.VMEM((8, 2 * GROUP_ROWS), f32),
            pltpu.VMEM((HEAD + 16, 2 * GROUP_ROWS), f32),
            pltpu.VMEM((GROUP_ROWS, 2 * HEAD), bf),
            pltpu.VMEM((Y * C, ROWS, 2 * HEAD), bf),
            pltpu.VMEM((Y * C, 2 * HEAD, D), bf),
            pltpu.VMEM((ROWS, D), f32),
            dma((15,)), dma((8,)), dma((8,)), dma((3,)), dma((3,)), dma((7,)), dma((7,)), dma((7,)), dma((7,)),
            dma((24,)), dma((24,)), dma((9,)), dma((9,)), dma((16,)), dma((16,)),
            dma((8,)), dma((8,)), dma((2,)), dma((2,)), dma((8,)), dma((8,)),
        ],
        compiler_params=pltpu.CompilerParams(collective_id=0, has_side_effects=True, vmem_limit_bytes=62 << 20),
    )(
        latents, context, cond.reshape(1, -1), ctx_cond.reshape(1, -1), mod_weight, wq, wk, wv, out_weight,
        q_gain.reshape(1, -1), k_gain.reshape(1, -1), *rope_tables(),
    )


def solution(mesh):
    torus = Mesh(mesh.devices.reshape(Z, X, Y, C), AXES)
    placed = (
        P(AXES, None), P(SP, None), P(SP), P(SP), P(SP, TP), P(None, TP), P(None, TP), P(None, TP),
        P(TP, None), P(), P(),
    )
    return jax.shard_map(layer, mesh=torus, in_specs=placed, out_specs=P(AXES, None), check_vma=False)
```

```python
import functools
import math

import jax
import jax.numpy as jnp
import numpy as np
from jax import lax
from jax.experimental import pallas as pl
from jax.experimental.pallas import tpu as pltpu
from jax.sharding import Mesh
from jax.sharding import PartitionSpec as P

GRID_W = 64
NORM_EPS = 1e-06
ROPE_BASE = 10000.0
Z, X, Y, C = 8, 4, 4, 2
AXES = ("z", "x", "y", "c")
SP = ("z", "x")
TP = ("y", "c")
MESH = pl.DeviceIdType.MESH
D = 2048
HEAD = 128
ROWS = 64
CTX_ROWS = 16
GROUP_ROWS = ROWS * Y * C
UNIT = CTX_ROWS + GROUP_ROWS
TOTAL_KEYS = UNIT * Z * X
LIFT = 16.0
SCORE_SCALE = HEAD ** (-0.5) * math.log2(math.e)


def coords():
    return tuple(lax.axis_index(a) for a in AXES)


def remote(src, dst, send, recv, dev):
    return pltpu.make_async_remote_copy(
        src_ref=src, dst_ref=dst, send_sem=send, recv_sem=recv, device_id=dev, device_id_type=MESH
    )


def meet(peers):
    barrier = pltpu.get_barrier_semaphore()
    for dev in peers:
        pl.semaphore_signal(barrier, inc=1, device_id=dev, device_id_type=MESH)
    pl.semaphore_wait(barrier, len(peers))


def rope_tables():
    quarter = HEAD // 4
    freq = (np.float32(ROPE_BASE) ** (-np.arange(quarter, dtype=np.float32) / np.float32(quarter))).astype(np.float32)
    lanes = freq[np.arange(HEAD) % quarter]
    sign = np.where(np.arange(HEAD) % (HEAD // 2) < quarter, -1.0, 1.0)
    grid_rows = GROUP_ROWS * Z * X // GRID_W
    row_angle = (np.arange(grid_rows, dtype=np.float32)[:, None] * lanes[None]).astype(np.float64)
    col_angle = (np.arange(GRID_W, dtype=np.float32)[:, None] * lanes[None]).astype(np.float64)
    as32 = lambda a: jnp.asarray(a.astype(np.float32))
    return (
        as32(np.cos(row_angle)),
        as32(np.sin(row_angle) * sign),
        as32(np.cos(col_angle)),
        as32(np.sin(col_angle) * sign),
    )


def column(row):
    n = row.shape[1]
    eye = lax.broadcasted_iota(jnp.int32, (n, n), 0) == lax.broadcasted_iota(jnp.int32, (n, n), 1)
    return jnp.sum(jnp.where(eye, row, 0.0), axis=1, keepdims=True)


H1 = 240
H2 = UNIT - H1
CHUNK = 1408
CHUNKS = TOTAL_KEYS // CHUNK
SUB = 352


def unit_order():
    order = [(0, "own", s) for s in (0, 1)] + [(0, "nbr", s) for s in (0, 1)]
    for t, col in ((1, "own"), (1, "nbr"), (2, "own"), (2, "nbr"), (3, "own"), (3, "nbr"), (4, "own"), (4, "nbr")):
        for s in (0, 1):
            order += [(d, col, s) for d in ((t, -t) if t < 4 else (4,))]
    return {u: i for i, u in enumerate(order)}


ORDER = unit_order()
DS = (0, 1, -1, 2, -2, 3, -3, 4)
KINDS = ("own", "nbr", "h2")


def layer_kernel(
    lat_in, ctx_in, cond_in, ctx_cond_in, modw_in, wq, wk, wv, ow_in, q_gain_in, k_gain_in, cos_r, sin_r, cos_c_in, sin_c_in,
    out,
    lat, ctx, cond, ctx_cond, modw, q_gain, k_gain, cos_c, sin_c, cr, sr,
    xg, wqs, wkv, part, x_in, x_sum, z_in, mod, xn, kvb, qt,
    keys, qb, ones, m_ref, acc, att, got, ow, mixed,
    loc, lat_send, lat_recv, mx_send, mx_recv, mz_send, mz_recv, mt_send, mt_recv,
    z_send, z_recv, x_send, x_recv, d_send, d_recv, o_send, o_recv, s_send, s_recv, a_send, a_recv,
):
    z, x, y, c = coords()
    me = y * C + c
    sp = z * X + x
    pair = x + 1 - 2 * lax.rem(x, 2)
    is_a = lax.rem((x + 1) // 2, 2)
    swapped = is_a == c
    row_x = x + (pair - x) * (1 - lax.rem(is_a + c, 2))
    head = y * C + 1 - is_a
    up, down, far = lax.rem(y + 1, Y), lax.rem(y + Y - 1, Y), lax.rem(y + 2, Y)
    sib = (z, x, y, 1 - c)
    partner = (z, pair, y, 1 - c)
    nbr = (z, X - 1 - x, y, c)
    z_up, z_down = (lax.rem(z + 1, Z), x, y, c), (lax.rem(z + Z - 1, Z), x, y, c)
    y_up, y_down = (z, x, up, c), (z, x, down, c)
    rel = [(ry, rc) for ry in range(Y) for rc in range(C)]
    flip = 1 - 2 * c
    x_peers = [(z, lax.rem(x + r, X), y, c) for r in range(1, X)]
    z_peers = [(lax.rem(z + r, Z), x, y, c) for r in range(1, Z)]
    t_peers = [(z, x, lax.rem(y + ry, Y), c + rc * flip) for ry, rc in rel[1:]]

    loads = [
        pltpu.make_async_copy(src, dst, loc.at[i])
        for i, (src, dst) in enumerate((
            (modw_in, modw), (cond_in, cond), (ctx_cond_in, ctx_cond), (lat_in, lat), (ctx_in, ctx),
            (q_gain_in, q_gain), (k_gain_in, k_gain), (cos_c_in, cos_c), (sin_c_in, sin_c),
            (cos_r.at[pl.ds(sp * 8, 8)], cr), (sin_r.at[pl.ds(sp * 8, 8)], sr),
            (wk, wkv.at[:, pl.ds(0, HEAD)]), (wv, wkv.at[:, pl.ds(HEAD, HEAD)]), (wq, wqs), (ow_in, ow.at[me]),
        ))
    ]
    for copy in loads:
        copy.start()
    meet(x_peers + z_peers + t_peers + [(z, pair, lax.rem(y + ry, Y), c + rc * flip) for ry, rc in rel[1:]])

    lat_sends = []

    def send_lat(i, src, yy, dev, lo=0, n=ROWS):
        copy = remote(src, xg.at[yy * C + c, pl.ds(lo, n)], lat_send.at[i], lat_recv.at[i], dev)
        copy.start()
        lat_sends.append(copy)
        return copy

    hr = ROWS // 2
    low, high = pl.ds(0, hr), pl.ds(hr, hr)
    up_a = send_lat(0, lat_in.at[low], y, y_up, 0, hr)
    down_a = send_lat(1, lat_in.at[high], y, y_down, hr, hr)
    up_b = send_lat(2, lat_in.at[high], y, y_up, hr, hr)
    down_b = send_lat(3, lat_in.at[low], y, y_down, 0, hr)
    own = send_lat(4, lat_in, y, sib)
    for copy in loads[:5]:
        copy.wait()

    w = modw[...]
    for r, vec in enumerate((cond, ctx_cond)):
        v = vec[...]
        v = column(v * lax.logistic(v))
        row = jnp.sum(v * w, axis=0, keepdims=True)
        for i in range(6):
            part[r * 6 + i : r * 6 + i + 1, :] = row[:, i * HEAD : (i + 1) * HEAD]
    part[12:16, :] = jnp.zeros((4, HEAD), jnp.float32)

    xs = [remote(part, x_in.at[i], mx_send.at[i], mx_recv.at[i], d) for i, d in enumerate(x_peers)]
    for s in xs:
        s.start()
    xg[me] = lat[...]
    wt = lax.broadcasted_iota(jnp.int32, ones.shape, 1)
    ones[...] = jnp.where(lax.rem(wt, UNIT) < CTX_ROWS, LIFT, 1.0).astype(jnp.bfloat16)
    m_ref[...] = jnp.full_like(m_ref, -1e30)
    acc[...] = jnp.zeros_like(acc)
    for s in xs:
        s.wait_recv()
    x_sum[...] = part[...] + x_in[0] + x_in[1] + x_in[2]
    zs = [remote(x_sum, z_in.at[i], mz_send.at[i], mz_recv.at[i], d) for i, d in enumerate(z_peers)]
    for s in zs:
        s.start()

    up_a.wait_recv()
    far_a = send_lat(5, xg.at[down * C + c, low], down, y_up, 0, hr)
    down_a.wait_recv()
    far_b = send_lat(6, xg.at[up * C + c, high], up, y_down, hr, hr)

    for s in zs:
        s.wait_recv()
    total = x_sum[...]
    for i in range(Z - 1):
        total = total + z_in[i]
    mod[me] = total
    ts = [remote(mod.at[me], mod.at[me], mt_send.at[i], mt_recv.at[i], d) for i, d in enumerate(t_peers)]
    for s in ts:
        s.start()
    up_b.wait_recv()
    from_down = send_lat(7, xg.at[down * C + c], down, sib)
    down_b.wait_recv()
    from_up = send_lat(8, xg.at[up * C + c], up, sib)
    for copy in loads[5:]:
        copy.wait()
    far_a.wait_recv()
    far_b.wait_recv()
    from_far = send_lat(9, xg.at[far * C + c], far, sib)
    for s in ts:
        s.wait_recv()

    def mod_row(r, first):
        tiles = [first + t for t in range(D // HEAD)]
        return jnp.concatenate([mod[t // 6, r * 6 + t % 6 : r * 6 + t % 6 + 1, :] for t in tiles], axis=1)

    def modulated(rows, r):
        v = rows.astype(jnp.float32)
        v = v * lax.rsqrt(jnp.mean(v * v, axis=-1, keepdims=True) + NORM_EPS)
        return (v * (1.0 + mod_row(r, 16)) + mod_row(r, 0)).astype(jnp.bfloat16)

    def make_rows(j):
        lo = pl.multiple_of(CTX_ROWS + ROWS * j, CTX_ROWS)
        xn[pl.ds(lo, ROWS), :] = modulated(xg[j], 0)

    xn[:CTX_ROWS, :] = modulated(ctx[...], 1)
    make_rows(me)
    own.wait_recv()
    make_rows(y * C + 1 - c)
    make_rows(down * C + c)
    make_rows(up * C + c)
    make_rows(far * C + c)
    from_down.wait_recv()
    make_rows(down * C + 1 - c)
    from_up.wait_recv()
    make_rows(up * C + 1 - c)
    from_far.wait_recv()
    make_rows(far * C + 1 - c)

    lane = lax.broadcasted_iota(jnp.int32, (GRID_W, HEAD), 1)
    is_row = lane < HEAD // 2
    is_first = lax.rem(lane, HEAD // 2) < HEAD // 4

    def unit_rows(v, gain):
        return v * lax.rsqrt(jnp.mean(v * v, axis=-1, keepdims=True) + NORM_EPS) * gain

    def turned(v, gain, j):
        cos = jnp.where(is_row, cr[j : j + 1, :], cos_c[...])
        sin = jnp.where(is_row, sr[j : j + 1, :], sin_c[...])
        v = unit_rows(v, gain)
        other = jnp.where(is_first, pltpu.roll(v, HEAD - HEAD // 4, 1), pltpu.roll(v, HEAD // 4, 1))
        return (v * cos + other * sin).astype(jnp.bfloat16)

    qg, kg = q_gain[...], k_gain[...]
    blocks = GROUP_ROWS // GRID_W

    def at(d, col, s, lo, n):
        return keys.at[pl.ds(ORDER[(d, col, s)] * UNIT + lo, n)]

    def swap_kv():
        return remote(kvb, keys.at[pl.ds(0, UNIT)], s_send.at[0], s_recv.at[0], partner)

    def swap_q():
        return remote(qt, qb, s_send.at[1], s_recv.at[1], partner)

    def ring(direction, t, kind):
        col = "nbr" if kind == "nbr" else "own"
        lo, n = (H1, H2) if kind == "h2" else (0, H1)
        if kind == "h2" and t == 4:
            n = H2 // 2
            lo = lo if direction > 0 else lo + n
        dst = 4 if t == 4 else direction * t
        i = (0 if direction > 0 else 12) + (t - 1) * 3 + KINDS.index(kind)
        return remote(
            at(direction * (t - 1), col, 0, lo, n), at(dst, col, 0, lo, n), z_send.at[i], z_recv.at[i],
            z_up if direction > 0 else z_down,
        )

    def used(direction, t, kind):
        return t < 4 or kind == "h2" or (kind == "own") == (direction > 0)

    def cross(d):
        i = DS.index(d)
        return remote(at(d, "own", 0, H1, H2), at(d, "nbr", 0, H1, H2), x_send.at[i], x_recv.at[i], nbr)

    def cross_h1():
        return remote(at(0, "own", 0, 0, H1), at(0, "nbr", 0, 0, H1), x_send.at[8], x_recv.at[8], nbr)

    def share(d, col):
        i = DS.index(d) + (0 if col == "own" else 8)
        return remote(at(d, col, 0, 0, UNIT), at(d, col, 1, 0, UNIT), d_send.at[i], d_recv.at[i], sib)

    half = 2 * HEAD // 2

    def weight(i):
        who = [
            (ow_in, me, 0, 2 * half, y_up), (ow_in, me, 0, 2 * half, y_down), (ow_in, me, 0, 2 * half, sib),
            (None, down * C + c, 0, half, y_up), (None, up * C + c, half, half, y_down),
            (None, down * C + c, 0, 2 * half, sib), (None, up * C + c, 0, 2 * half, sib),
            (None, far * C + c, 0, 2 * half, sib),
        ][i]
        src, slot, lo, n, dev = who
        dst = ow.at[slot, pl.ds(lo, n)]
        return remote(dst if src is None else src, dst, o_send.at[i], o_recv.at[i], dev)

    def on_ring(t, kind):
        for direction in (1, -1):
            if used(direction, t, kind):
                ring(direction, t, kind).wait_recv()
            if t < 4 and used(direction, t + 1, kind):
                ring(direction, t + 1, kind).start()


    for i in range(3):
        weight(i).start()
    proj = jnp.dot(xn[...], wkv[...], preferred_element_type=jnp.float32)
    kvb[:CTX_ROWS, :HEAD] = unit_rows(proj[:CTX_ROWS, :HEAD], kg).astype(jnp.bfloat16)
    kvb[:CTX_ROWS, HEAD:] = proj[:CTX_ROWS, HEAD:].astype(jnp.bfloat16) * jnp.bfloat16(LIFT)
    for j in range(blocks):
        lo = CTX_ROWS + GRID_W * j
        kvb[lo : lo + GRID_W, :HEAD] = turned(proj[lo : lo + GRID_W, :HEAD], kg, j)
        kvb[lo : lo + GRID_W, HEAD:] = proj[lo : lo + GRID_W, HEAD:].astype(jnp.bfloat16)

    @pl.when(swapped)
    def _():
        swap_kv().start()

    @pl.when(jnp.logical_not(swapped))
    def _():
        keys[:UNIT, :] = kvb[...]

    def launch():
        cross_h1().start()
        for kind in ("h2", "own"):
            for direction in (1, -1):
                ring(direction, 1, kind).start()
        cross(0).start()
        share(0, "own").start()

    @pl.when(jnp.logical_not(swapped))
    def _():
        launch()

    proj = jnp.dot(xn[CTX_ROWS:, :], wqs[...], preferred_element_type=jnp.float32)
    for j in range(blocks):
        lo = GRID_W * j
        for h in range(2):
            qt[h * GROUP_ROWS + lo : h * GROUP_ROWS + lo + GRID_W, :] = turned(
                proj[lo : lo + GRID_W, h * HEAD : (h + 1) * HEAD], qg, j
            )

    @pl.when(swapped)
    def _():
        swap_q().start()
        swap_kv().wait_recv()
        launch()

    @pl.when(jnp.logical_not(swapped))
    def _():
        qb[...] = qt[...]

    def both(t):
        return (t, -t) if 0 < t < 4 else (t,)

    def h2_in(t):
        on_ring(t, "h2")
        for d in both(t):
            cross(d).start()

    def own_in(t):
        on_ring(t, "own")
        for d in both(t):
            share(d, "own").start()

    def nbr_in(t):
        for d in both(t):
            cross(d).wait_recv()
            share(d, "nbr").start()

    def shared(t, col):
        for d in both(t):
            share(d, col).wait_recv()

    def before0():
        cross_h1().wait_recv()
        for direction in (1, -1):
            ring(direction, 1, "nbr").start()
        h2_in(1)
        own_in(1)
        nbr_in(0)

        @pl.when(swapped)
        def _():
            swap_q().wait_recv()

        shared(0, "own")

    def before1():
        shared(0, "nbr")
        on_ring(1, "nbr")

    def before2():
        shared(1, "own")

    def within2():
        h2_in(2)
        nbr_in(1)

    def before3():
        shared(1, "nbr")

    def within3():
        own_in(2)
        for i in (0, 1):
            weight(i).wait_recv()
        for i in (3, 4, 5, 6):
            weight(i).start()

    def within4():
        on_ring(2, "nbr")

    def before5():
        shared(2, "own")

    def within5():
        h2_in(3)
        nbr_in(2)

    def before6():
        shared(2, "nbr")

    def within6():
        own_in(3)

    def within7():
        on_ring(3, "nbr")

    def before8():
        shared(3, "own")

    def within8():
        h2_in(4)
        nbr_in(3)

    def before9():
        shared(3, "nbr")

    def within9():
        own_in(4)
        on_ring(4, "nbr")

    def before10():
        shared(4, "own")

    def within10():
        nbr_in(4)
        for i in (3, 4):
            weight(i).wait_recv()
        weight(7).start()

    def before11():
        shared(4, "nbr")

    before = {0: before0, 1: before1, 2: before2, 3: before3, 5: before5, 6: before6, 8: before8, 9: before9,
              10: before10, 11: before11}
    within = {2: within2, 3: within3, 4: within4, 5: within5, 6: within6, 7: within7, 8: within8, 9: within9,
              10: within10}

    def chunk(i, carry):
        for j, step in before.items():
            pl.when(i == j)(step)
        rows = pl.ds(pl.multiple_of(i * CHUNK, CHUNK), CHUNK)
        k = keys[rows, :HEAD]
        q = qb[...]
        scores = [
            lax.dot_general(k[a : a + SUB], q, (((1,), (1,)), ((), ())), preferred_element_type=jnp.float32)
            for a in range(0, CHUNK, SUB)
        ]
        weights = ones[:, pl.ds(pl.multiple_of(lax.rem(i, 3) * CHUNK, HEAD), CHUNK)]
        v = jnp.concatenate([keys[rows, HEAD:].T, weights], axis=0)
        m_old = m_ref[0:1, :]
        m_new = m_old
        for s in scores:
            m_new = jnp.maximum(m_new, jnp.max(s, axis=0, keepdims=True))
        for j, step in within.items():
            pl.when(i == j)(step)
        p = jnp.concatenate([jnp.exp2((s - m_new) * SCORE_SCALE).astype(jnp.bfloat16) for s in scores], axis=0)
        fade = jnp.exp2((m_old - m_new) * SCORE_SCALE)
        acc[...] = acc[...] * fade + jnp.dot(v, p, preferred_element_type=jnp.float32)
        m_ref[...] = jnp.broadcast_to(m_new, m_ref.shape)
        return carry

    lax.fori_loop(0, CHUNKS, chunk, 0)

    for h in range(2):
        sl = pl.ds(h * GROUP_ROWS, GROUP_ROWS)
        att[:, h * HEAD : (h + 1) * HEAD] = (acc[:HEAD, sl] / acc[HEAD : HEAD + 1, sl]).T.astype(jnp.bfloat16)

    def hand(i):
        ry, rc = rel[i]
        yy, cc = lax.rem(y + ry, Y), c + rc * flip
        src = att.at[pl.ds(pl.multiple_of((yy * C + cc) * ROWS, ROWS), ROWS)]
        return remote(src, got.at[head], a_send.at[i], a_recv.at[head], (z, row_x, yy, cc))

    for i in range(1, Y * C):
        hand(i).start()

    @pl.when(swapped)
    def _():
        hand(0).start()

    @pl.when(jnp.logical_not(swapped))
    def _():
        got[head] = att[pl.ds(pl.multiple_of(me * ROWS, ROWS), ROWS), :]

    for i in (2, 5, 6, 7):
        weight(i).wait_recv()
    for j in range(Y * C):

        @pl.when(jnp.logical_or(swapped, head != j))
        def _():
            remote(att.at[pl.ds(0, ROWS)], got.at[j], a_send.at[0], a_recv.at[j], sib).wait_recv()

    rows = jnp.concatenate([got[j] for j in range(Y * C)], axis=1)
    for n in range(0, D, 512):
        total = jnp.zeros((ROWS, 512), jnp.float32)
        for j in range(Y * C):
            total = total + jnp.dot(
                rows[:, j * 2 * HEAD : (j + 1) * 2 * HEAD], ow[j, :, n : n + 512], preferred_element_type=jnp.float32
            )
        mixed[:, n : n + 512] = total
    v = mixed[...]
    v = v * lax.rsqrt(jnp.mean(v * v, axis=-1, keepdims=True) + NORM_EPS)
    out[...] = (lat[...].astype(jnp.float32) + mod_row(0, 32) * v).astype(jnp.bfloat16)

    for kind in KINDS:
        for t in range(1, 5):
            for direction in (1, -1):
                if used(direction, t, kind):
                    ring(direction, t, kind).wait_send()
    for d in DS:
        cross(d).wait_send()
        share(d, "own").wait_send()
        share(d, "nbr").wait_send()
    cross_h1().wait_send()
    for i in range(8):
        weight(i).wait_send()
    for i in range(1, Y * C):
        hand(i).wait_send()


    for s in lat_sends + xs + zs + ts:
        s.wait_send()

    @pl.when(swapped)
    def _():
        hand(0).wait_send()
        swap_kv().wait_send()
        swap_q().wait_send()


def layer(latents, context, cond, ctx_cond, mod_weight, wq, wk, wv, out_weight, q_gain, k_gain):
    hbm = pl.BlockSpec(memory_space=pltpu.HBM)
    bf, f32 = jnp.bfloat16, jnp.float32
    dma = pltpu.SemaphoreType.DMA
    return pl.pallas_call(
        layer_kernel,
        name="layer",
        out_shape=jax.ShapeDtypeStruct((ROWS, D), bf),
        in_specs=[hbm] * 15,
        out_specs=pl.BlockSpec(memory_space=pltpu.VMEM),
        scratch_shapes=[
            pltpu.VMEM((ROWS, D), bf),
            pltpu.VMEM((CTX_ROWS, D), bf),
            pltpu.VMEM((1, ROWS), f32),
            pltpu.VMEM((1, ROWS), f32),
            pltpu.VMEM((ROWS, 6 * HEAD), f32),
            pltpu.VMEM((1, HEAD), f32),
            pltpu.VMEM((1, HEAD), f32),
            pltpu.VMEM((GRID_W, HEAD), f32),
            pltpu.VMEM((GRID_W, HEAD), f32),
            pltpu.VMEM((8, HEAD), f32),
            pltpu.VMEM((8, HEAD), f32),
            pltpu.VMEM((Y * C, ROWS, D), bf),
            pltpu.VMEM((D, 2 * HEAD), bf),
            pltpu.VMEM((D, 2 * HEAD), bf),
            pltpu.VMEM((16, HEAD), f32),
            pltpu.VMEM((X - 1, 16, HEAD), f32),
            pltpu.VMEM((16, HEAD), f32),
            pltpu.VMEM((Z - 1, 16, HEAD), f32),
            pltpu.VMEM((Y * C, 16, HEAD), f32),
            pltpu.VMEM((UNIT, D), bf),
            pltpu.VMEM((UNIT, 2 * HEAD), bf),
            pltpu.VMEM((2 * GROUP_ROWS, HEAD), bf),
            pltpu.VMEM((TOTAL_KEYS, 2 * HEAD), bf),
            pltpu.VMEM((2 * GROUP_ROWS, HEAD), bf),
            pltpu.VMEM((16, 3 * CHUNK), bf),
            pltpu.VMEM((8, 2 * GROUP_ROWS), f32),
            pltpu.VMEM((HEAD + 16, 2 * GROUP_ROWS), f32),
            pltpu.VMEM((GROUP_ROWS, 2 * HEAD), bf),
            pltpu.VMEM((Y * C, ROWS, 2 * HEAD), bf),
            pltpu.VMEM((Y * C, 2 * HEAD, D), bf),
            pltpu.VMEM((ROWS, D), f32),
            dma((15,)), dma((10,)), dma((10,)), dma((3,)), dma((3,)), dma((7,)), dma((7,)), dma((7,)), dma((7,)),
            dma((24,)), dma((24,)), dma((9,)), dma((9,)), dma((16,)), dma((16,)),
            dma((8,)), dma((8,)), dma((2,)), dma((2,)), dma((8,)), dma((8,)),
        ],
        compiler_params=pltpu.CompilerParams(collective_id=0, has_side_effects=True, vmem_limit_bytes=62 << 20),
    )(
        latents, context, cond.reshape(1, -1), ctx_cond.reshape(1, -1), mod_weight, wq, wk, wv, out_weight,
        q_gain.reshape(1, -1), k_gain.reshape(1, -1), *rope_tables(),
    )


def solution(mesh):
    torus = Mesh(mesh.devices.reshape(Z, X, Y, C), AXES)
    placed = (
        P(AXES, None), P(SP, None), P(SP), P(SP), P(SP, TP), P(None, TP), P(None, TP), P(None, TP),
        P(TP, None), P(), P(),
    )
    return jax.shard_map(layer, mesh=torus, in_specs=placed, out_specs=P(AXES, None), check_vma=False)
```

```python
import functools
import math

import jax
import jax.numpy as jnp
import numpy as np
from jax import lax
from jax.experimental import pallas as pl
from jax.experimental.pallas import tpu as pltpu
from jax.sharding import Mesh
from jax.sharding import PartitionSpec as P

GRID_W = 64
NORM_EPS = 1e-06
ROPE_BASE = 10000.0
Z, X, Y, C = 8, 4, 4, 2
AXES = ("z", "x", "y", "c")
SP = ("z", "x")
TP = ("y", "c")
MESH = pl.DeviceIdType.MESH
D = 2048
HEAD = 128
ROWS = 64
CTX_ROWS = 16
GROUP_ROWS = ROWS * Y * C
UNIT = CTX_ROWS + GROUP_ROWS
TOTAL_KEYS = UNIT * Z * X
LIFT = 16.0
SCORE_SCALE = HEAD ** (-0.5) * math.log2(math.e)


def coords():
    return tuple(lax.axis_index(a) for a in AXES)


def remote(src, dst, send, recv, dev):
    return pltpu.make_async_remote_copy(
        src_ref=src, dst_ref=dst, send_sem=send, recv_sem=recv, device_id=dev, device_id_type=MESH
    )


def meet(peers):
    barrier = pltpu.get_barrier_semaphore()
    for dev in peers:
        pl.semaphore_signal(barrier, inc=1, device_id=dev, device_id_type=MESH)
    pl.semaphore_wait(barrier, len(peers))


def rope_tables():
    quarter = HEAD // 4
    freq = (np.float32(ROPE_BASE) ** (-np.arange(quarter, dtype=np.float32) / np.float32(quarter))).astype(np.float32)
    lanes = freq[np.arange(HEAD) % quarter]
    sign = np.where(np.arange(HEAD) % (HEAD // 2) < quarter, -1.0, 1.0)
    grid_rows = GROUP_ROWS * Z * X // GRID_W
    row_angle = (np.arange(grid_rows, dtype=np.float32)[:, None] * lanes[None]).astype(np.float64)
    col_angle = (np.arange(GRID_W, dtype=np.float32)[:, None] * lanes[None]).astype(np.float64)
    as32 = lambda a: jnp.asarray(a.astype(np.float32))
    return (
        as32(np.cos(row_angle)),
        as32(np.sin(row_angle) * sign),
        as32(np.cos(col_angle)),
        as32(np.sin(col_angle) * sign),
    )


def column(row):
    n = row.shape[1]
    eye = lax.broadcasted_iota(jnp.int32, (n, n), 0) == lax.broadcasted_iota(jnp.int32, (n, n), 1)
    return jnp.sum(jnp.where(eye, row, 0.0), axis=1, keepdims=True)


H1 = 240
H2 = UNIT - H1
CHUNK = 1408
CHUNKS = TOTAL_KEYS // CHUNK
SUB = 352


def unit_order():
    order = [(0, "own", s) for s in (0, 1)] + [(0, "nbr", s) for s in (0, 1)]
    for t, col in ((1, "own"), (1, "nbr"), (2, "own"), (2, "nbr"), (3, "own"), (3, "nbr"), (4, "own"), (4, "nbr")):
        for s in (0, 1):
            order += [(d, col, s) for d in ((t, -t) if t < 4 else (4,))]
    return {u: i for i, u in enumerate(order)}


ORDER = unit_order()
DS = (0, 1, -1, 2, -2, 3, -3, 4)
KINDS = ("own", "nbr", "h2")


def layer_kernel(
    lat_in, ctx_in, cond_in, ctx_cond_in, modw_in, wq, wk, wv, ow_in, q_gain_in, k_gain_in, cos_r, sin_r, cos_c_in, sin_c_in,
    out,
    lat, ctx, cond, ctx_cond, modw, q_gain, k_gain, cos_c, sin_c, cr, sr,
    xg, wqs, wkv, part, x_in, x_sum, z_in, mod, xn, kvb, qt,
    keys, qb, ones, m_ref, acc, att, got, ow, mixed,
    loc, lat_send, lat_recv, mx_send, mx_recv, mz_send, mz_recv, mt_send, mt_recv,
    z_send, z_recv, x_send, x_recv, d_send, d_recv, o_send, o_recv, s_send, s_recv, a_send, a_recv,
):
    z, x, y, c = coords()
    me = y * C + c
    sp = z * X + x
    pair = x + 1 - 2 * lax.rem(x, 2)
    is_a = lax.rem((x + 1) // 2, 2)
    swapped = is_a == c
    row_x = x + (pair - x) * (1 - lax.rem(is_a + c, 2))
    head = y * C + 1 - is_a
    up, down, far = lax.rem(y + 1, Y), lax.rem(y + Y - 1, Y), lax.rem(y + 2, Y)
    sib = (z, x, y, 1 - c)
    partner = (z, pair, y, 1 - c)
    nbr = (z, X - 1 - x, y, c)
    z_up, z_down = (lax.rem(z + 1, Z), x, y, c), (lax.rem(z + Z - 1, Z), x, y, c)
    y_up, y_down = (z, x, up, c), (z, x, down, c)
    rel = [(ry, rc) for ry in range(Y) for rc in range(C)]
    flip = 1 - 2 * c
    x_peers = [(z, lax.rem(x + r, X), y, c) for r in range(1, X)]
    z_peers = [(lax.rem(z + r, Z), x, y, c) for r in range(1, Z)]
    t_peers = [(z, x, lax.rem(y + ry, Y), c + rc * flip) for ry, rc in rel[1:]]

    loads = [
        pltpu.make_async_copy(src, dst, loc.at[i])
        for i, (src, dst) in enumerate((
            (modw_in, modw), (cond_in, cond), (ctx_cond_in, ctx_cond), (lat_in, lat), (ctx_in, ctx),
            (q_gain_in, q_gain), (k_gain_in, k_gain), (cos_c_in, cos_c), (sin_c_in, sin_c),
            (cos_r.at[pl.ds(sp * 8, 8)], cr), (sin_r.at[pl.ds(sp * 8, 8)], sr),
            (wk, wkv.at[:, pl.ds(0, HEAD)]), (wv, wkv.at[:, pl.ds(HEAD, HEAD)]), (wq, wqs), (ow_in, ow.at[me]),
        ))
    ]
    for copy in loads:
        copy.start()
    meet(x_peers + z_peers + t_peers + [(z, pair, lax.rem(y + ry, Y), c + rc * flip) for ry, rc in rel[1:]])

    lat_sends = []

    def send_lat(i, src, yy, dev, lo=0, n=ROWS):
        copy = remote(src, xg.at[yy * C + c, pl.ds(lo, n)], lat_send.at[i], lat_recv.at[i], dev)
        copy.start()
        lat_sends.append(copy)
        return copy

    hr = ROWS // 2
    low, high = pl.ds(0, hr), pl.ds(hr, hr)
    up_a = send_lat(0, lat_in.at[low], y, y_up, 0, hr)
    down_a = send_lat(1, lat_in.at[high], y, y_down, hr, hr)
    up_b = send_lat(2, lat_in.at[high], y, y_up, hr, hr)
    down_b = send_lat(3, lat_in.at[low], y, y_down, 0, hr)
    own = send_lat(4, lat_in, y, sib)
    for copy in loads[:5]:
        copy.wait()

    w = modw[...]
    for r, vec in enumerate((cond, ctx_cond)):
        v = vec[...]
        v = column(v * lax.logistic(v))
        row = jnp.sum(v * w, axis=0, keepdims=True)
        for i in range(6):
            part[r * 6 + i : r * 6 + i + 1, :] = row[:, i * HEAD : (i + 1) * HEAD]
    part[12:16, :] = jnp.zeros((4, HEAD), jnp.float32)

    xs = [remote(part, x_in.at[i], mx_send.at[i], mx_recv.at[i], d) for i, d in enumerate(x_peers)]
    for s in xs:
        s.start()
    xg[me] = lat[...]
    wt = lax.broadcasted_iota(jnp.int32, ones.shape, 1)
    ones[...] = jnp.where(lax.rem(wt, UNIT) < CTX_ROWS, LIFT, 1.0).astype(jnp.bfloat16)
    m_ref[...] = jnp.full_like(m_ref, -1e30)
    acc[...] = jnp.zeros_like(acc)
    for s in xs:
        s.wait_recv()
    x_sum[...] = part[...] + x_in[0] + x_in[1] + x_in[2]
    zs = [remote(x_sum, z_in.at[i], mz_send.at[i], mz_recv.at[i], d) for i, d in enumerate(z_peers)]
    for s in zs:
        s.start()

    up_a.wait_recv()
    far_a = send_lat(5, xg.at[down * C + c, low], down, y_up, 0, hr)
    down_a.wait_recv()
    far_b = send_lat(6, xg.at[up * C + c, high], up, y_down, hr, hr)

    for s in zs:
        s.wait_recv()
    total = x_sum[...]
    for i in range(Z - 1):
        total = total + z_in[i]
    mod[me] = total
    ts = [remote(mod.at[me], mod.at[me], mt_send.at[i], mt_recv.at[i], d) for i, d in enumerate(t_peers)]
    for s in ts:
        s.start()
    up_b.wait_recv()
    from_down = send_lat(7, xg.at[down * C + c], down, sib)
    down_b.wait_recv()
    from_up = send_lat(8, xg.at[up * C + c], up, sib)
    for copy in loads[5:]:
        copy.wait()
    far_a.wait_recv()
    far_b.wait_recv()
    from_far = send_lat(9, xg.at[far * C + c], far, sib)
    for s in ts:
        s.wait_recv()

    def mod_row(r, first):
        tiles = [first + t for t in range(D // HEAD)]
        return jnp.concatenate([mod[t // 6, r * 6 + t % 6 : r * 6 + t % 6 + 1, :] for t in tiles], axis=1)

    def modulated(rows, r):
        v = rows.astype(jnp.float32)
        v = v * lax.rsqrt(jnp.mean(v * v, axis=-1, keepdims=True) + NORM_EPS)
        return (v * (1.0 + mod_row(r, 16)) + mod_row(r, 0)).astype(jnp.bfloat16)

    def make_rows(j):
        lo = pl.multiple_of(CTX_ROWS + ROWS * j, CTX_ROWS)
        xn[pl.ds(lo, ROWS), :] = modulated(xg[j], 0)

    xn[:CTX_ROWS, :] = modulated(ctx[...], 1)
    make_rows(me)
    own.wait_recv()
    make_rows(y * C + 1 - c)
    make_rows(down * C + c)
    make_rows(up * C + c)
    make_rows(far * C + c)
    from_down.wait_recv()
    make_rows(down * C + 1 - c)
    from_up.wait_recv()
    make_rows(up * C + 1 - c)
    from_far.wait_recv()
    make_rows(far * C + 1 - c)

    piece = GRID_W // 2
    lane = lax.broadcasted_iota(jnp.int32, (piece, HEAD), 1)
    is_row = lane < HEAD // 2
    is_first = lax.rem(lane, HEAD // 2) < HEAD // 4

    def unit_rows(v, gain):
        return v * lax.rsqrt(jnp.mean(v * v, axis=-1, keepdims=True) + NORM_EPS) * gain

    def turned(v, gain, row):
        j, o, n = row // GRID_W, row % GRID_W, v.shape[0]
        cos = jnp.where(is_row, cr[j : j + 1, :], cos_c[o : o + n, :])
        sin = jnp.where(is_row, sr[j : j + 1, :], sin_c[o : o + n, :])
        v = unit_rows(v, gain)
        other = jnp.where(is_first, pltpu.roll(v, HEAD - HEAD // 4, 1), pltpu.roll(v, HEAD // 4, 1))
        return (v * cos + other * sin).astype(jnp.bfloat16)

    qg, kg = q_gain[...], k_gain[...]

    def at(d, col, s, lo, n):
        return keys.at[pl.ds(ORDER[(d, col, s)] * UNIT + lo, n)]

    parts = {"h1": pl.ds(0, H1), "h2": pl.ds(H1, H2)}

    def swap_kv(part):
        i = 0 if part == "h1" else 2
        return remote(kvb.at[parts[part]], keys.at[parts[part]], s_send.at[i], s_recv.at[i], partner)

    def swap_q():
        return remote(qt, qb, s_send.at[1], s_recv.at[1], partner)

    def ring(direction, t, kind):
        col = "nbr" if kind == "nbr" else "own"
        lo, n = (H1, H2) if kind == "h2" else (0, H1)
        if kind == "h2" and t == 4:
            n = H2 // 2
            lo = lo if direction > 0 else lo + n
        dst = 4 if t == 4 else direction * t
        i = (0 if direction > 0 else 12) + (t - 1) * 3 + KINDS.index(kind)
        return remote(
            at(direction * (t - 1), col, 0, lo, n), at(dst, col, 0, lo, n), z_send.at[i], z_recv.at[i],
            z_up if direction > 0 else z_down,
        )

    def used(direction, t, kind):
        return t < 4 or kind == "h2" or (kind == "own") == (direction > 0)

    def cross(d):
        i = DS.index(d)
        return remote(at(d, "own", 0, H1, H2), at(d, "nbr", 0, H1, H2), x_send.at[i], x_recv.at[i], nbr)

    def cross_h1():
        return remote(at(0, "own", 0, 0, H1), at(0, "nbr", 0, 0, H1), x_send.at[8], x_recv.at[8], nbr)

    def share(d, col):
        i = DS.index(d) + (0 if col == "own" else 8)
        return remote(at(d, col, 0, 0, UNIT), at(d, col, 1, 0, UNIT), d_send.at[i], d_recv.at[i], sib)

    half = 2 * HEAD // 2

    def weight(i):
        who = [
            (ow_in, me, 0, 2 * half, y_up), (ow_in, me, 0, 2 * half, y_down), (ow_in, me, 0, 2 * half, sib),
            (None, down * C + c, 0, half, y_up), (None, up * C + c, half, half, y_down),
            (None, down * C + c, 0, 2 * half, sib), (None, up * C + c, 0, 2 * half, sib),
            (None, far * C + c, 0, 2 * half, sib),
        ][i]
        src, slot, lo, n, dev = who
        dst = ow.at[slot, pl.ds(lo, n)]
        return remote(dst if src is None else src, dst, o_send.at[i], o_recv.at[i], dev)

    def on_ring(t, kind):
        for direction in (1, -1):
            if used(direction, t, kind):
                ring(direction, t, kind).wait_recv()
            if t < 4 and used(direction, t + 1, kind):
                ring(direction, t + 1, kind).start()


    for i in range(3):
        weight(i).start()

    def make_kv(lo, hi):
        proj = jnp.dot(xn[lo:hi, :], wkv[...], preferred_element_type=jnp.float32)
        if lo == 0:
            kvb[:CTX_ROWS, :HEAD] = unit_rows(proj[:CTX_ROWS, :HEAD], kg).astype(jnp.bfloat16)
            kvb[:CTX_ROWS, HEAD:] = proj[:CTX_ROWS, HEAD:].astype(jnp.bfloat16) * jnp.bfloat16(LIFT)
        for r in range(max(lo, CTX_ROWS), hi, piece):
            rows = proj[r - lo : r - lo + piece]
            kvb[r : r + piece, :HEAD] = turned(rows[:, :HEAD], kg, r - CTX_ROWS)
            kvb[r : r + piece, HEAD:] = rows[:, HEAD:].astype(jnp.bfloat16)

    def launch(part):
        if part == "h1":
            cross_h1().start()
        for direction in (1, -1):
            ring(direction, 1, "own" if part == "h1" else "h2").start()
        if part == "h1":
            cross(0).start()
            share(0, "own").start()

    for part, lo, hi in (("h2", H1, UNIT), ("h1", 0, H1)):
        make_kv(lo, hi)

        @pl.when(swapped)
        def _():
            swap_kv(part).start()

        @pl.when(jnp.logical_not(swapped))
        def _():
            keys[lo:hi, :] = kvb[lo:hi, :]
            launch(part)

    proj = jnp.dot(xn[CTX_ROWS:, :], wqs[...], preferred_element_type=jnp.float32)
    for r in range(0, GROUP_ROWS, piece):
        for h in range(2):
            qt[h * GROUP_ROWS + r : h * GROUP_ROWS + r + piece, :] = turned(
                proj[r : r + piece, h * HEAD : (h + 1) * HEAD], qg, r
            )

    @pl.when(swapped)
    def _():
        swap_q().start()
        for part in ("h2", "h1"):
            swap_kv(part).wait_recv()
            launch(part)

    @pl.when(jnp.logical_not(swapped))
    def _():
        qb[...] = qt[...]

    def both(t):
        return (t, -t) if 0 < t < 4 else (t,)

    def h2_in(t):
        on_ring(t, "h2")
        for d in both(t):
            cross(d).start()

    def own_in(t):
        on_ring(t, "own")
        for d in both(t):
            share(d, "own").start()

    def nbr_in(t):
        for d in both(t):
            cross(d).wait_recv()
            share(d, "nbr").start()

    def shared(t, col):
        for d in both(t):
            share(d, col).wait_recv()

    def before0():
        cross_h1().wait_recv()
        for direction in (1, -1):
            ring(direction, 1, "nbr").start()
        h2_in(1)
        own_in(1)
        nbr_in(0)

        @pl.when(swapped)
        def _():
            swap_q().wait_recv()

        shared(0, "own")

    def before1():
        shared(0, "nbr")

    def within1():
        on_ring(1, "nbr")

    def before2():
        shared(1, "own")

    def within2():
        h2_in(2)
        nbr_in(1)

    def before3():
        shared(1, "nbr")

    def within3():
        own_in(2)

    def within4():
        on_ring(2, "nbr")
        for i in (0, 1):
            weight(i).wait_recv()
        for i in (3, 4, 5, 6):
            weight(i).start()

    def before5():
        shared(2, "own")

    def within5():
        h2_in(3)
        nbr_in(2)

    def before6():
        shared(2, "nbr")

    def within6():
        own_in(3)

    def within7():
        on_ring(3, "nbr")

    def before8():
        shared(3, "own")

    def within8():
        h2_in(4)
        nbr_in(3)

    def before9():
        shared(3, "nbr")

    def within9():
        own_in(4)
        on_ring(4, "nbr")

    def before10():
        shared(4, "own")

    def within10():
        nbr_in(4)
        for i in (3, 4):
            weight(i).wait_recv()
        weight(7).start()

    def before11():
        shared(4, "nbr")

    before = {0: before0, 1: before1, 2: before2, 3: before3, 5: before5, 6: before6, 8: before8, 9: before9,
              10: before10}
    within = {1: within1, 2: within2, 3: within3, 4: within4, 5: within5, 6: within6, 7: within7, 8: within8, 9: within9,
              10: within10}

    def flash(i, sl, between):
        rows = pl.ds(pl.multiple_of(i * CHUNK, CHUNK), CHUNK)
        k = keys[rows, :HEAD]
        q = qb[sl, :]
        scores = [
            lax.dot_general(k[a : a + SUB], q, (((1,), (1,)), ((), ())), preferred_element_type=jnp.float32)
            for a in range(0, CHUNK, SUB)
        ]
        weights = ones[:, pl.ds(pl.multiple_of(lax.rem(i, 3) * CHUNK, HEAD), CHUNK)]
        v = jnp.concatenate([keys[rows, HEAD:].T, weights], axis=0)
        m_old = m_ref[0:1, sl]
        m_new = m_old
        for s in scores:
            m_new = jnp.maximum(m_new, jnp.max(s, axis=0, keepdims=True))
        between()
        p = jnp.concatenate([jnp.exp2((s - m_new) * SCORE_SCALE).astype(jnp.bfloat16) for s in scores], axis=0)
        fade = jnp.exp2((m_old - m_new) * SCORE_SCALE)
        total = acc[:, sl] * fade + jnp.dot(v, p, preferred_element_type=jnp.float32)
        return total, m_new

    def chunk(i, carry):
        for j, step in before.items():
            pl.when(i == j)(step)

        def between():
            for j, step in within.items():
                pl.when(i == j)(step)

        total, m_new = flash(i, pl.ds(0, 2 * GROUP_ROWS), between)
        acc[...] = total
        m_ref[...] = jnp.broadcast_to(m_new, m_ref.shape)
        return carry

    lax.fori_loop(0, CHUNKS - 1, chunk, 0)
    before11()

    def hand(i, h):
        ry, rc = rel[i]
        yy, cc = lax.rem(y + ry, Y), c + rc * flip
        src = att.at[h, pl.ds(pl.multiple_of((yy * C + cc) * ROWS, ROWS), ROWS)]
        return remote(src, got.at[h, head], a_send.at[h, i], a_recv.at[h, head], (z, row_x, yy, cc))

    far_first = sorted(range(1, Y * C), key=lambda i: -min(rel[i][0], Y - rel[i][0]))
    for h in range(2):
        total, _ = flash(CHUNKS - 1, pl.ds(h * GROUP_ROWS, GROUP_ROWS), lambda: None)
        att[h] = (total[:HEAD] / total[HEAD : HEAD + 1]).T.astype(jnp.bfloat16)
        for i in far_first:
            hand(i, h).start()

        @pl.when(swapped)
        def _():
            hand(0, h).start()

        @pl.when(jnp.logical_not(swapped))
        def _():
            got[h, head] = att[h, pl.ds(pl.multiple_of(me * ROWS, ROWS), ROWS), :]

    for i in (2, 5, 6, 7):
        weight(i).wait_recv()
    for j in range(Y * C):

        @pl.when(jnp.logical_or(swapped, head != j))
        def _():
            for h in range(2):
                remote(att.at[h, pl.ds(0, ROWS)], got.at[h, j], a_send.at[h, 0], a_recv.at[h, j], sib).wait_recv()

    rows = jnp.concatenate([got[h, j] for j in range(Y * C) for h in range(2)], axis=1)
    for n in range(0, D, 512):
        total = jnp.zeros((ROWS, 512), jnp.float32)
        for j in range(Y * C):
            total = total + jnp.dot(
                rows[:, j * 2 * HEAD : (j + 1) * 2 * HEAD], ow[j, :, n : n + 512], preferred_element_type=jnp.float32
            )
        mixed[:, n : n + 512] = total
    v = mixed[...]
    v = v * lax.rsqrt(jnp.mean(v * v, axis=-1, keepdims=True) + NORM_EPS)
    out[...] = (lat[...].astype(jnp.float32) + mod_row(0, 32) * v).astype(jnp.bfloat16)

    for kind in KINDS:
        for t in range(1, 5):
            for direction in (1, -1):
                if used(direction, t, kind):
                    ring(direction, t, kind).wait_send()
    for d in DS:
        cross(d).wait_send()
        share(d, "own").wait_send()
        share(d, "nbr").wait_send()
    cross_h1().wait_send()
    for i in range(8):
        weight(i).wait_send()
    for i in range(1, Y * C):
        hand(i, 0).wait_send()
        hand(i, 1).wait_send()


    for s in lat_sends + xs + zs + ts:
        s.wait_send()

    @pl.when(swapped)
    def _():
        hand(0, 0).wait_send()
        hand(0, 1).wait_send()
        swap_kv("h1").wait_send()
        swap_kv("h2").wait_send()
        swap_q().wait_send()


def layer(latents, context, cond, ctx_cond, mod_weight, wq, wk, wv, out_weight, q_gain, k_gain):
    hbm = pl.BlockSpec(memory_space=pltpu.HBM)
    bf, f32 = jnp.bfloat16, jnp.float32
    dma = pltpu.SemaphoreType.DMA
    return pl.pallas_call(
        layer_kernel,
        name="layer",
        out_shape=jax.ShapeDtypeStruct((ROWS, D), bf),
        in_specs=[hbm] * 15,
        out_specs=pl.BlockSpec(memory_space=pltpu.VMEM),
        scratch_shapes=[
            pltpu.VMEM((ROWS, D), bf),
            pltpu.VMEM((CTX_ROWS, D), bf),
            pltpu.VMEM((1, ROWS), f32),
            pltpu.VMEM((1, ROWS), f32),
            pltpu.VMEM((ROWS, 6 * HEAD), f32),
            pltpu.VMEM((1, HEAD), f32),
            pltpu.VMEM((1, HEAD), f32),
            pltpu.VMEM((GRID_W, HEAD), f32),
            pltpu.VMEM((GRID_W, HEAD), f32),
            pltpu.VMEM((8, HEAD), f32),
            pltpu.VMEM((8, HEAD), f32),
            pltpu.VMEM((Y * C, ROWS, D), bf),
            pltpu.VMEM((D, 2 * HEAD), bf),
            pltpu.VMEM((D, 2 * HEAD), bf),
            pltpu.VMEM((16, HEAD), f32),
            pltpu.VMEM((X - 1, 16, HEAD), f32),
            pltpu.VMEM((16, HEAD), f32),
            pltpu.VMEM((Z - 1, 16, HEAD), f32),
            pltpu.VMEM((Y * C, 16, HEAD), f32),
            pltpu.VMEM((UNIT, D), bf),
            pltpu.VMEM((UNIT, 2 * HEAD), bf),
            pltpu.VMEM((2 * GROUP_ROWS, HEAD), bf),
            pltpu.VMEM((TOTAL_KEYS, 2 * HEAD), bf),
            pltpu.VMEM((2 * GROUP_ROWS, HEAD), bf),
            pltpu.VMEM((16, 3 * CHUNK), bf),
            pltpu.VMEM((8, 2 * GROUP_ROWS), f32),
            pltpu.VMEM((HEAD + 16, 2 * GROUP_ROWS), f32),
            pltpu.VMEM((2, GROUP_ROWS, HEAD), bf),
            pltpu.VMEM((2, Y * C, ROWS, HEAD), bf),
            pltpu.VMEM((Y * C, 2 * HEAD, D), bf),
            pltpu.VMEM((ROWS, D), f32),
            dma((15,)), dma((10,)), dma((10,)), dma((3,)), dma((3,)), dma((7,)), dma((7,)), dma((7,)), dma((7,)),
            dma((24,)), dma((24,)), dma((9,)), dma((9,)), dma((16,)), dma((16,)),
            dma((8,)), dma((8,)), dma((3,)), dma((3,)), dma((2, 8)), dma((2, 8)),
        ],
        compiler_params=pltpu.CompilerParams(collective_id=0, has_side_effects=True, vmem_limit_bytes=62 << 20),
    )(
        latents, context, cond.reshape(1, -1), ctx_cond.reshape(1, -1), mod_weight, wq, wk, wv, out_weight,
        q_gain.reshape(1, -1), k_gain.reshape(1, -1), *rope_tables(),
    )


def solution(mesh):
    torus = Mesh(mesh.devices.reshape(Z, X, Y, C), AXES)
    placed = (
        P(AXES, None), P(SP, None), P(SP), P(SP), P(SP, TP), P(None, TP), P(None, TP), P(None, TP),
        P(TP, None), P(), P(),
    )
    return jax.shard_map(layer, mesh=torus, in_specs=placed, out_specs=P(AXES, None), check_vma=False)
```

```python
import functools
import math

import jax
import jax.numpy as jnp
import numpy as np
from jax import lax
from jax.experimental import pallas as pl
from jax.experimental.pallas import tpu as pltpu
from jax.sharding import Mesh
from jax.sharding import PartitionSpec as P

GRID_W = 64
NORM_EPS = 1e-06
ROPE_BASE = 10000.0
Z, X, Y, C = 8, 4, 4, 2
AXES = ("z", "x", "y", "c")
SP = ("z", "x")
TP = ("y", "c")
MESH = pl.DeviceIdType.MESH
D = 2048
HEAD = 128
ROWS = 64
CTX_ROWS = 16
GROUP_ROWS = ROWS * Y * C
UNIT = CTX_ROWS + GROUP_ROWS
TOTAL_KEYS = UNIT * Z * X
LIFT = 16.0
SCORE_SCALE = HEAD ** (-0.5) * math.log2(math.e)


def coords():
    return tuple(lax.axis_index(a) for a in AXES)


def remote(src, dst, send, recv, dev):
    return pltpu.make_async_remote_copy(
        src_ref=src, dst_ref=dst, send_sem=send, recv_sem=recv, device_id=dev, device_id_type=MESH
    )


def meet(peers):
    barrier = pltpu.get_barrier_semaphore()
    for dev in peers:
        pl.semaphore_signal(barrier, inc=1, device_id=dev, device_id_type=MESH)
    pl.semaphore_wait(barrier, len(peers))


def rope_tables():
    quarter = HEAD // 4
    freq = (np.float32(ROPE_BASE) ** (-np.arange(quarter, dtype=np.float32) / np.float32(quarter))).astype(np.float32)
    lanes = freq[np.arange(HEAD) % quarter]
    sign = np.where(np.arange(HEAD) % (HEAD // 2) < quarter, -1.0, 1.0)
    grid_rows = GROUP_ROWS * Z * X // GRID_W
    row_angle = (np.arange(grid_rows, dtype=np.float32)[:, None] * lanes[None]).astype(np.float64)
    col_angle = (np.arange(GRID_W, dtype=np.float32)[:, None] * lanes[None]).astype(np.float64)
    as32 = lambda a: jnp.asarray(a.astype(np.float32))
    return (
        as32(np.cos(row_angle)),
        as32(np.sin(row_angle) * sign),
        as32(np.cos(col_angle)),
        as32(np.sin(col_angle) * sign),
    )


def column(row):
    n = row.shape[1]
    eye = lax.broadcasted_iota(jnp.int32, (n, n), 0) == lax.broadcasted_iota(jnp.int32, (n, n), 1)
    return jnp.sum(jnp.where(eye, row, 0.0), axis=1, keepdims=True)


H1 = 240
H2 = UNIT - H1
CHUNK = 1408
CHUNKS = TOTAL_KEYS // CHUNK
SUB = 352


def unit_order():
    order = [(0, "own", s) for s in (0, 1)] + [(0, "nbr", s) for s in (0, 1)]
    for t, col in ((1, "own"), (1, "nbr"), (2, "own"), (2, "nbr"), (3, "own"), (3, "nbr"), (4, "own"), (4, "nbr")):
        for s in (0, 1):
            order += [(d, col, s) for d in ((t, -t) if t < 4 else (4,))]
    return {u: i for i, u in enumerate(order)}


ORDER = unit_order()
DS = (0, 1, -1, 2, -2, 3, -3, 4)
KINDS = ("own", "nbr", "h2")


def layer_kernel(
    lat_in, ctx_in, cond_in, ctx_cond_in, modw_in, wq, wk, wv, ow_in, q_gain_in, k_gain_in, cos_r, sin_r, cos_c_in, sin_c_in,
    out,
    lat, ctx, cond, ctx_cond, modw, q_gain, k_gain, cos_c, sin_c, cr, sr,
    xg, wqs, wkv, part, x_in, x_sum, z_in, mod, xn, kvb, qt,
    keys, qb, ones, m_ref, acc, att, got, ow, mixed,
    loc, lat_send, lat_recv, mx_send, mx_recv, mz_send, mz_recv, mt_send, mt_recv,
    z_send, z_recv, x_send, x_recv, d_send, d_recv, o_send, o_recv, s_send, s_recv, a_send, a_recv,
):
    z, x, y, c = coords()
    me = y * C + c
    sp = z * X + x
    pair = x + 1 - 2 * lax.rem(x, 2)
    is_a = lax.rem((x + 1) // 2, 2)
    swapped = is_a == c
    row_x = x + (pair - x) * (1 - lax.rem(is_a + c, 2))
    head = y * C + 1 - is_a
    up, down, far = lax.rem(y + 1, Y), lax.rem(y + Y - 1, Y), lax.rem(y + 2, Y)
    sib = (z, x, y, 1 - c)
    partner = (z, pair, y, 1 - c)
    nbr = (z, X - 1 - x, y, c)
    z_up, z_down = (lax.rem(z + 1, Z), x, y, c), (lax.rem(z + Z - 1, Z), x, y, c)
    y_up, y_down = (z, x, up, c), (z, x, down, c)
    rel = [(ry, rc) for ry in range(Y) for rc in range(C)]
    flip = 1 - 2 * c
    x_peers = [(z, lax.rem(x + r, X), y, c) for r in range(1, X)]
    z_peers = [(lax.rem(z + r, Z), x, y, c) for r in range(1, Z)]
    t_peers = [(z, x, lax.rem(y + ry, Y), c + rc * flip) for ry, rc in rel[1:]]

    loads = [
        pltpu.make_async_copy(src, dst, loc.at[i])
        for i, (src, dst) in enumerate((
            (modw_in, modw), (cond_in, cond), (ctx_cond_in, ctx_cond), (lat_in, lat), (ctx_in, ctx),
            (q_gain_in, q_gain), (k_gain_in, k_gain), (cos_c_in, cos_c), (sin_c_in, sin_c),
            (cos_r.at[pl.ds(sp * 8, 8)], cr), (sin_r.at[pl.ds(sp * 8, 8)], sr),
            (wk, wkv.at[:, pl.ds(0, HEAD)]), (wv, wkv.at[:, pl.ds(HEAD, HEAD)]), (wq, wqs), (ow_in, ow.at[me]),
        ))
    ]
    for copy in loads:
        copy.start()
    meet(x_peers + z_peers + t_peers + [(z, pair, lax.rem(y + ry, Y), c + rc * flip) for ry, rc in rel[1:]])

    lat_sends = []

    def send_lat(i, src, yy, dev, lo=0, n=ROWS):
        copy = remote(src, xg.at[yy * C + c, pl.ds(lo, n)], lat_send.at[i], lat_recv.at[i], dev)
        copy.start()
        lat_sends.append(copy)
        return copy

    hr = ROWS // 2
    low, high = pl.ds(0, hr), pl.ds(hr, hr)
    up_a = send_lat(0, lat_in.at[low], y, y_up, 0, hr)
    down_a = send_lat(1, lat_in.at[high], y, y_down, hr, hr)
    up_b = send_lat(2, lat_in.at[high], y, y_up, hr, hr)
    down_b = send_lat(3, lat_in.at[low], y, y_down, 0, hr)
    own = send_lat(4, lat_in, y, sib)
    for copy in loads[:5]:
        copy.wait()

    w = modw[...]
    for r, vec in enumerate((cond, ctx_cond)):
        v = vec[...]
        v = column(v * lax.logistic(v))
        row = jnp.sum(v * w, axis=0, keepdims=True)
        for i in range(6):
            part[r * 6 + i : r * 6 + i + 1, :] = row[:, i * HEAD : (i + 1) * HEAD]
    part[12:16, :] = jnp.zeros((4, HEAD), jnp.float32)

    xs = [remote(part, x_in.at[i], mx_send.at[i], mx_recv.at[i], d) for i, d in enumerate(x_peers)]
    for s in xs:
        s.start()
    xg[me] = lat[...]
    wt = lax.broadcasted_iota(jnp.int32, ones.shape, 1)
    ones[...] = jnp.where(lax.rem(wt, UNIT) < CTX_ROWS, LIFT, 1.0).astype(jnp.bfloat16)
    m_ref[...] = jnp.full_like(m_ref, -1e30)
    acc[...] = jnp.zeros_like(acc)
    for s in xs:
        s.wait_recv()
    x_sum[...] = part[...] + x_in[0] + x_in[1] + x_in[2]
    zs = [remote(x_sum, z_in.at[i], mz_send.at[i], mz_recv.at[i], d) for i, d in enumerate(z_peers)]
    for s in zs:
        s.start()

    up_a.wait_recv()
    far_a = send_lat(5, xg.at[down * C + c, low], down, y_up, 0, hr)
    down_a.wait_recv()
    far_b = send_lat(6, xg.at[up * C + c, high], up, y_down, hr, hr)

    for s in zs:
        s.wait_recv()
    total = x_sum[...]
    for i in range(Z - 1):
        total = total + z_in[i]
    mod[me] = total
    ts = [remote(mod.at[me], mod.at[me], mt_send.at[i], mt_recv.at[i], d) for i, d in enumerate(t_peers)]
    for s in ts:
        s.start()
    up_b.wait_recv()
    from_down = send_lat(7, xg.at[down * C + c], down, sib)
    down_b.wait_recv()
    from_up = send_lat(8, xg.at[up * C + c], up, sib)
    for copy in loads[5:]:
        copy.wait()
    far_a.wait_recv()
    far_b.wait_recv()
    from_far = send_lat(9, xg.at[far * C + c], far, sib)
    for s in ts:
        s.wait_recv()

    def mod_row(r, first):
        tiles = [first + t for t in range(D // HEAD)]
        return jnp.concatenate([mod[t // 6, r * 6 + t % 6 : r * 6 + t % 6 + 1, :] for t in tiles], axis=1)

    def modulated(rows, r):
        v = rows.astype(jnp.float32)
        v = v * lax.rsqrt(jnp.mean(v * v, axis=-1, keepdims=True) + NORM_EPS)
        return (v * (1.0 + mod_row(r, 16)) + mod_row(r, 0)).astype(jnp.bfloat16)

    def make_rows(j):
        lo = pl.multiple_of(CTX_ROWS + ROWS * j, CTX_ROWS)
        xn[pl.ds(lo, ROWS), :] = modulated(xg[j], 0)

    xn[:CTX_ROWS, :] = modulated(ctx[...], 1)
    make_rows(me)
    own.wait_recv()
    make_rows(y * C + 1 - c)
    make_rows(down * C + c)
    make_rows(up * C + c)
    make_rows(far * C + c)
    from_down.wait_recv()
    make_rows(down * C + 1 - c)
    from_up.wait_recv()
    make_rows(up * C + 1 - c)
    from_far.wait_recv()
    make_rows(far * C + 1 - c)

    piece = GRID_W // 2
    lane = lax.broadcasted_iota(jnp.int32, (piece, HEAD), 1)
    is_row = lane < HEAD // 2
    is_first = lax.rem(lane, HEAD // 2) < HEAD // 4

    def unit_rows(v, gain):
        return v * lax.rsqrt(jnp.mean(v * v, axis=-1, keepdims=True) + NORM_EPS) * gain

    def turned(v, gain, row):
        j, o, n = row // GRID_W, row % GRID_W, v.shape[0]
        cos = jnp.where(is_row, cr[j : j + 1, :], cos_c[o : o + n, :])
        sin = jnp.where(is_row, sr[j : j + 1, :], sin_c[o : o + n, :])
        v = unit_rows(v, gain)
        other = jnp.where(is_first, pltpu.roll(v, HEAD - HEAD // 4, 1), pltpu.roll(v, HEAD // 4, 1))
        return (v * cos + other * sin).astype(jnp.bfloat16)

    qg, kg = q_gain[...], k_gain[...]

    late = 1 - lax.rem(is_a + c, 2)

    def at(d, col, s, lo, n):
        if d == 0 and col == "nbr":
            place = 2 + (1 - late if s else late)
            return keys.at[pl.ds(pl.multiple_of(place * UNIT + lo, CTX_ROWS), n)]
        return keys.at[pl.ds(ORDER[(d, col, s)] * UNIT + lo, n)]

    parts = {"h1": pl.ds(0, H1), "h2": pl.ds(H1, H2)}

    def swap_kv(part):
        i = 0 if part == "h1" else 2
        return remote(kvb.at[parts[part]], keys.at[parts[part]], s_send.at[i], s_recv.at[i], partner)

    def swap_q():
        return remote(qt, qb, s_send.at[1], s_recv.at[1], partner)

    def ring(direction, t, kind):
        col = "nbr" if kind == "nbr" else "own"
        lo, n = (H1, H2) if kind == "h2" else (0, H1)
        if kind == "h2" and t == 4:
            n = H2 // 2
            lo = lo if direction > 0 else lo + n
        dst = 4 if t == 4 else direction * t
        i = (0 if direction > 0 else 12) + (t - 1) * 3 + KINDS.index(kind)
        return remote(
            at(direction * (t - 1), col, 0, lo, n), at(dst, col, 0, lo, n), z_send.at[i], z_recv.at[i],
            z_up if direction > 0 else z_down,
        )

    def used(direction, t, kind):
        return t < 4 or kind == "h2" or (kind == "own") == (direction > 0)

    def cross(d):
        i = DS.index(d)
        return remote(at(d, "own", 0, H1, H2), at(d, "nbr", 0, H1, H2), x_send.at[i], x_recv.at[i], nbr)

    def cross_h1():
        return remote(at(0, "own", 0, 0, H1), at(0, "nbr", 0, 0, H1), x_send.at[8], x_recv.at[8], nbr)

    def share(d, col):
        i = DS.index(d) + (0 if col == "own" else 8)
        there = 0 if d == 0 and col == "nbr" else 1
        return remote(at(d, col, 0, 0, UNIT), at(d, col, there, 0, UNIT), d_send.at[i], d_recv.at[i], sib)

    half = 2 * HEAD // 2

    def weight(i):
        who = [
            (ow_in, me, 0, 2 * half, y_up), (ow_in, me, 0, 2 * half, y_down), (ow_in, me, 0, 2 * half, sib),
            (None, down * C + c, 0, half, y_up), (None, up * C + c, half, half, y_down),
            (None, down * C + c, 0, 2 * half, sib), (None, up * C + c, 0, 2 * half, sib),
            (None, far * C + c, 0, 2 * half, sib),
        ][i]
        src, slot, lo, n, dev = who
        dst = ow.at[slot, pl.ds(lo, n)]
        return remote(dst if src is None else src, dst, o_send.at[i], o_recv.at[i], dev)

    def on_ring(t, kind):
        for direction in (1, -1):
            if used(direction, t, kind):
                ring(direction, t, kind).wait_recv()
            if t < 4 and used(direction, t + 1, kind):
                ring(direction, t + 1, kind).start()


    for i in range(3):
        weight(i).start()

    def make_kv(lo, hi):
        proj = jnp.dot(xn[lo:hi, :], wkv[...], preferred_element_type=jnp.float32)
        if lo == 0:
            kvb[:CTX_ROWS, :HEAD] = unit_rows(proj[:CTX_ROWS, :HEAD], kg).astype(jnp.bfloat16)
            kvb[:CTX_ROWS, HEAD:] = proj[:CTX_ROWS, HEAD:].astype(jnp.bfloat16) * jnp.bfloat16(LIFT)
        for r in range(max(lo, CTX_ROWS), hi, piece):
            rows = proj[r - lo : r - lo + piece]
            kvb[r : r + piece, :HEAD] = turned(rows[:, :HEAD], kg, r - CTX_ROWS)
            kvb[r : r + piece, HEAD:] = rows[:, HEAD:].astype(jnp.bfloat16)

    def launch(part):
        if part == "h1":
            cross_h1().start()
        for direction in (1, -1):
            ring(direction, 1, "own" if part == "h1" else "h2").start()
        if part == "h1":
            cross(0).start()
            share(0, "own").start()

    for part, lo, hi in (("h2", H1, UNIT), ("h1", 0, H1)):
        make_kv(lo, hi)

        @pl.when(swapped)
        def _():
            swap_kv(part).start()

        @pl.when(jnp.logical_not(swapped))
        def _():
            keys[lo:hi, :] = kvb[lo:hi, :]
            launch(part)

    proj = jnp.dot(xn[CTX_ROWS:, :], wqs[...], preferred_element_type=jnp.float32)
    for r in range(0, GROUP_ROWS, piece):
        for h in range(2):
            qt[h * GROUP_ROWS + r : h * GROUP_ROWS + r + piece, :] = turned(
                proj[r : r + piece, h * HEAD : (h + 1) * HEAD], qg, r
            )

    @pl.when(swapped)
    def _():
        swap_q().start()
        for part in ("h2", "h1"):
            swap_kv(part).wait_recv()
            launch(part)

    @pl.when(jnp.logical_not(swapped))
    def _():
        qb[...] = qt[...]

    def both(t):
        return (t, -t) if 0 < t < 4 else (t,)

    def h2_in(t):
        on_ring(t, "h2")
        for d in both(t):
            cross(d).start()

    def own_in(t):
        on_ring(t, "own")
        for d in both(t):
            share(d, "own").start()

    def nbr_in(t):
        for d in both(t):
            cross(d).wait_recv()
            share(d, "nbr").start()

    def shared(t, col):
        for d in both(t):
            share(d, col).wait_recv()

    def before0():
        cross_h1().wait_recv()
        for direction in (1, -1):
            ring(direction, 1, "nbr").start()

        @pl.when(jnp.logical_not(swapped))
        def _():
            h2_in(1)
            own_in(1)
            nbr_in(0)

        @pl.when(swapped)
        def _():
            swap_q().wait_recv()
            shared(0, "nbr")

        shared(0, "own")

    def within0():
        @pl.when(swapped)
        def _():
            h2_in(1)
            own_in(1)
            nbr_in(0)

    def before1():
        @pl.when(jnp.logical_not(swapped))
        def _():
            shared(0, "nbr")

    def within1():
        on_ring(1, "nbr")

    def before2():
        shared(1, "own")

    def within2():
        h2_in(2)
        nbr_in(1)

    def before3():
        shared(1, "nbr")

    def within3():
        own_in(2)

    def within4():
        on_ring(2, "nbr")
        for i in (0, 1):
            weight(i).wait_recv()
        for i in (3, 4, 5, 6):
            weight(i).start()

    def before5():
        shared(2, "own")

    def within5():
        h2_in(3)
        nbr_in(2)

    def before6():
        shared(2, "nbr")

    def within6():
        own_in(3)

    def within7():
        on_ring(3, "nbr")

    def before8():
        shared(3, "own")

    def within8():
        h2_in(4)
        nbr_in(3)

    def before9():
        shared(3, "nbr")

    def within9():
        own_in(4)
        on_ring(4, "nbr")

    def before10():
        shared(4, "own")

    def within10():
        nbr_in(4)
        for i in (3, 4):
            weight(i).wait_recv()
        weight(7).start()

    def before11():
        shared(4, "nbr")

    before = {0: before0, 1: before1, 2: before2, 3: before3, 5: before5, 6: before6, 8: before8, 9: before9,
              10: before10}
    within = {0: within0, 1: within1, 2: within2, 3: within3, 4: within4, 5: within5, 6: within6, 7: within7, 8: within8, 9: within9,
              10: within10}

    def flash(i, sl, between):
        rows = pl.ds(pl.multiple_of(i * CHUNK, CHUNK), CHUNK)
        k = keys[rows, :HEAD]
        q = qb[sl, :]
        scores = [
            lax.dot_general(k[a : a + SUB], q, (((1,), (1,)), ((), ())), preferred_element_type=jnp.float32)
            for a in range(0, CHUNK, SUB)
        ]
        weights = ones[:, pl.ds(pl.multiple_of(lax.rem(i, 3) * CHUNK, HEAD), CHUNK)]
        v = jnp.concatenate([keys[rows, HEAD:].T, weights], axis=0)
        m_old = m_ref[0:1, sl]
        m_new = m_old
        for s in scores:
            m_new = jnp.maximum(m_new, jnp.max(s, axis=0, keepdims=True))
        between()
        p = jnp.concatenate([jnp.exp2((s - m_new) * SCORE_SCALE).astype(jnp.bfloat16) for s in scores], axis=0)
        fade = jnp.exp2((m_old - m_new) * SCORE_SCALE)
        total = acc[:, sl] * fade + jnp.dot(v, p, preferred_element_type=jnp.float32)
        return total, m_new

    def chunk(i, carry):
        for j, step in before.items():
            pl.when(i == j)(step)

        def between():
            for j, step in within.items():
                pl.when(i == j)(step)

        total, m_new = flash(i, pl.ds(0, 2 * GROUP_ROWS), between)
        acc[...] = total
        m_ref[...] = jnp.broadcast_to(m_new, m_ref.shape)
        return carry

    lax.fori_loop(0, CHUNKS - 1, chunk, 0)
    before11()

    def hand(i, h):
        ry, rc = rel[i]
        yy, cc = lax.rem(y + ry, Y), c + rc * flip
        src = att.at[h, pl.ds(pl.multiple_of((yy * C + cc) * ROWS, ROWS), ROWS)]
        return remote(src, got.at[h, head], a_send.at[h, i], a_recv.at[h, head], (z, row_x, yy, cc))

    far_first = sorted(range(1, Y * C), key=lambda i: -min(rel[i][0], Y - rel[i][0]))
    for h in range(2):
        total, _ = flash(CHUNKS - 1, pl.ds(h * GROUP_ROWS, GROUP_ROWS), lambda: None)
        att[h] = (total[:HEAD] / total[HEAD : HEAD + 1]).T.astype(jnp.bfloat16)
        for i in far_first:
            hand(i, h).start()

        @pl.when(swapped)
        def _():
            hand(0, h).start()

        @pl.when(jnp.logical_not(swapped))
        def _():
            got[h, head] = att[h, pl.ds(pl.multiple_of(me * ROWS, ROWS), ROWS), :]

    for i in (2, 5, 6, 7):
        weight(i).wait_recv()
    for j in range(Y * C):

        @pl.when(jnp.logical_or(swapped, head != j))
        def _():
            for h in range(2):
                remote(att.at[h, pl.ds(0, ROWS)], got.at[h, j], a_send.at[h, 0], a_recv.at[h, j], sib).wait_recv()

    rows = jnp.concatenate([got[h, j] for j in range(Y * C) for h in range(2)], axis=1)
    for n in range(0, D, 512):
        total = jnp.zeros((ROWS, 512), jnp.float32)
        for j in range(Y * C):
            total = total + jnp.dot(
                rows[:, j * 2 * HEAD : (j + 1) * 2 * HEAD], ow[j, :, n : n + 512], preferred_element_type=jnp.float32
            )
        mixed[:, n : n + 512] = total
    v = mixed[...]
    v = v * lax.rsqrt(jnp.mean(v * v, axis=-1, keepdims=True) + NORM_EPS)
    out[...] = (lat[...].astype(jnp.float32) + mod_row(0, 32) * v).astype(jnp.bfloat16)

    for kind in KINDS:
        for t in range(1, 5):
            for direction in (1, -1):
                if used(direction, t, kind):
                    ring(direction, t, kind).wait_send()
    for d in DS:
        cross(d).wait_send()
        share(d, "own").wait_send()
        share(d, "nbr").wait_send()
    cross_h1().wait_send()
    for i in range(8):
        weight(i).wait_send()
    for i in range(1, Y * C):
        hand(i, 0).wait_send()
        hand(i, 1).wait_send()


    for s in lat_sends + xs + zs + ts:
        s.wait_send()

    @pl.when(swapped)
    def _():
        hand(0, 0).wait_send()
        hand(0, 1).wait_send()
        swap_kv("h1").wait_send()
        swap_kv("h2").wait_send()
        swap_q().wait_send()


def layer(latents, context, cond, ctx_cond, mod_weight, wq, wk, wv, out_weight, q_gain, k_gain):
    hbm = pl.BlockSpec(memory_space=pltpu.HBM)
    bf, f32 = jnp.bfloat16, jnp.float32
    dma = pltpu.SemaphoreType.DMA
    return pl.pallas_call(
        layer_kernel,
        name="layer",
        out_shape=jax.ShapeDtypeStruct((ROWS, D), bf),
        in_specs=[hbm] * 15,
        out_specs=pl.BlockSpec(memory_space=pltpu.VMEM),
        scratch_shapes=[
            pltpu.VMEM((ROWS, D), bf),
            pltpu.VMEM((CTX_ROWS, D), bf),
            pltpu.VMEM((1, ROWS), f32),
            pltpu.VMEM((1, ROWS), f32),
            pltpu.VMEM((ROWS, 6 * HEAD), f32),
            pltpu.VMEM((1, HEAD), f32),
            pltpu.VMEM((1, HEAD), f32),
            pltpu.VMEM((GRID_W, HEAD), f32),
            pltpu.VMEM((GRID_W, HEAD), f32),
            pltpu.VMEM((8, HEAD), f32),
            pltpu.VMEM((8, HEAD), f32),
            pltpu.VMEM((Y * C, ROWS, D), bf),
            pltpu.VMEM((D, 2 * HEAD), bf),
            pltpu.VMEM((D, 2 * HEAD), bf),
            pltpu.VMEM((16, HEAD), f32),
            pltpu.VMEM((X - 1, 16, HEAD), f32),
            pltpu.VMEM((16, HEAD), f32),
            pltpu.VMEM((Z - 1, 16, HEAD), f32),
            pltpu.VMEM((Y * C, 16, HEAD), f32),
            pltpu.VMEM((UNIT, D), bf),
            pltpu.VMEM((UNIT, 2 * HEAD), bf),
            pltpu.VMEM((2 * GROUP_ROWS, HEAD), bf),
            pltpu.VMEM((TOTAL_KEYS, 2 * HEAD), bf),
            pltpu.VMEM((2 * GROUP_ROWS, HEAD), bf),
            pltpu.VMEM((16, 3 * CHUNK), bf),
            pltpu.VMEM((8, 2 * GROUP_ROWS), f32),
            pltpu.VMEM((HEAD + 16, 2 * GROUP_ROWS), f32),
            pltpu.VMEM((2, GROUP_ROWS, HEAD), bf),
            pltpu.VMEM((2, Y * C, ROWS, HEAD), bf),
            pltpu.VMEM((Y * C, 2 * HEAD, D), bf),
            pltpu.VMEM((ROWS, D), f32),
            dma((15,)), dma((10,)), dma((10,)), dma((3,)), dma((3,)), dma((7,)), dma((7,)), dma((7,)), dma((7,)),
            dma((24,)), dma((24,)), dma((9,)), dma((9,)), dma((16,)), dma((16,)),
            dma((8,)), dma((8,)), dma((3,)), dma((3,)), dma((2, 8)), dma((2, 8)),
        ],
        compiler_params=pltpu.CompilerParams(collective_id=0, has_side_effects=True, vmem_limit_bytes=62 << 20),
    )(
        latents, context, cond.reshape(1, -1), ctx_cond.reshape(1, -1), mod_weight, wq, wk, wv, out_weight,
        q_gain.reshape(1, -1), k_gain.reshape(1, -1), *rope_tables(),
    )


def solution(mesh):
    torus = Mesh(mesh.devices.reshape(Z, X, Y, C), AXES)
    placed = (
        P(AXES, None), P(SP, None), P(SP), P(SP), P(SP, TP), P(None, TP), P(None, TP), P(None, TP),
        P(TP, None), P(), P(),
    )
    return jax.shard_map(layer, mesh=torus, in_specs=placed, out_specs=P(AXES, None), check_vma=False)
```
